32 devices in a mesh: fs: 8 (over z, y), tp: 4 (over x, core).
Axes of the slice: x: 2, y: 2, z: 4, core: 2. Of those that a mesh axis runs over, the one named last changes fastest.
Arguments:
- tokens: bfloat16 [8, 384, 2048], P('fs', None, 'tp'), may hold values from -16 to 16
- first_gate: bfloat16 [2048, 6144], P('fs', 'tp'), may hold values from -0.125 to 0.125
- first_up: bfloat16 [2048, 6144], P('fs', 'tp'), may hold values from -0.125 to 0.125
- first_down: bfloat16 [6144, 2048], P('tp', 'fs'), may hold values from -0.078125 to 0.078125
- first_gain: bfloat16 [2048], P('tp'), may hold values from 0.099609375 to 1.8984375
- glu_value: bfloat16 [2048, 1024], P('fs', 'tp'), may hold values from -0.125 to 0.125
- glu_gate: bfloat16 [2048, 1024], P('fs', 'tp'), may hold values from -0.125 to 0.125
- conv_taps: bfloat16 [31, 1024], P(None, 'tp'), may hold values from -3 to 3
- conv_gain: bfloat16 [1024], P('tp'), may hold values from 0.099609375 to 1.8984375
- conv_proj: bfloat16 [1024, 2048], P('tp', 'fs'), may hold values from -0.1875 to 0.1875
- second_gain: bfloat16 [2048], P('tp'), may hold values from 0.099609375 to 1.8984375
- last_gate: bfloat16 [2048, 6144], P('fs', 'tp'), may hold values from -0.125 to 0.125
- last_up: bfloat16 [2048, 6144], P('fs', 'tp'), may hold values from -0.125 to 0.125
- last_down: bfloat16 [6144, 2048], P('tp', 'fs'), may hold values from -0.078125 to 0.078125
- third_gain: bfloat16 [2048], P('tp'), may hold values from 0.099609375 to 1.8984375
Outputs:
- layer_out: bfloat16 [8, 384, 2048], P('fs', None, 'tp')
The draws below stay inside these ranges and needn't reach their ends.
All inputs are finite; a program needn't handle non-finite values.
Results may differ from the reference program's by a relative error of at most 0.015.
Values may be sent and summed in bfloat16 or wider, within the bound.
A program may use at most 64 MiB of HBM per device.

```python
import jax
import jax.numpy as jnp
from jax import lax

D = 2048
FF = 6144
CONV = 1024
KERNEL = 31
LEN = 384
SEQS = 8
N_TP = 4


def draw_tokens(key, part):
    values = jnp.clip(jax.random.normal(key, (SEQS, LEN, D), jnp.float32), -5.0, 5.0)
    rising = 10.0 ** (jnp.arange(D, dtype=jnp.float32) / D - 0.5)
    return (values * rising).astype(jnp.bfloat16)


def draw_conv_taps(key, part):
    values = jnp.clip(jax.random.normal(key, (KERNEL, CONV), jnp.float32), -5.0, 5.0)
    rising = 10.0 ** (jnp.arange(CONV, dtype=jnp.float32) / CONV - 0.5)
    return (values * rising / jnp.sqrt(1.0 * KERNEL)).astype(jnp.bfloat16)


def shard_levels(own_key, extent, pieces, low, high):
    level, own = 1.0, jax.random.fold_in(own_key, 6)
    for axis_at, blocks in pieces:
        heights = jnp.exp(jax.random.uniform(jax.random.fold_in(own, axis_at), (blocks,), jnp.float32, low / len(pieces), high / len(pieces)))
        level = level * jnp.repeat(heights, extent[axis_at] // blocks).reshape([-1 if axis == axis_at else 1 for axis in range(len(extent))])
    return level


def centred(stream_key, extent, scale, bound, pieces=(), kind=jnp.bfloat16):
    values = scale * jax.random.normal(stream_key, extent, jnp.float32)
    if pieces:
        values = values * shard_levels(stream_key, extent, pieces, -0.22, 0.18)
    return jnp.clip(values, -bound, bound).astype(kind)


def setup_inputs(seed: int = 0) -> dict:
    streams_of = jax.random.split(jax.random.key(seed), 16)
    tokens = draw_tokens(jax.random.fold_in(streams_of[15], 71), 0)
    first_gate = centred(streams_of[1], (D, FF), D ** -0.5, 0.125, ((0, 8), (1, 4)))
    first_up = centred(streams_of[2], (D, FF), D ** -0.5, 0.125, ((0, 8), (1, 4)))
    first_down = centred(streams_of[3], (FF, D), FF ** -0.5, 0.078125, ((0, 4), (1, 8)))
    first_gain = jnp.clip(1.0 + 0.18 * jax.random.normal(streams_of[4], (D,), jnp.float32), 0.099609375, 1.8984375).astype(jnp.bfloat16)
    glu_value = centred(streams_of[5], (D, CONV), D ** -0.5, 0.125, ((0, 8), (1, 4)))
    glu_gate = centred(streams_of[6], (D, CONV), D ** -0.5, 0.125, ((0, 8), (1, 4)))
    conv_taps = draw_conv_taps(jax.random.fold_in(streams_of[15], 71), 0)
    conv_gain = jnp.clip(1.0 + 0.18 * jax.random.normal(streams_of[8], (CONV,), jnp.float32), 0.099609375, 1.8984375).astype(jnp.bfloat16)
    conv_proj = centred(streams_of[9], (CONV, D), CONV ** -0.5, 0.1875, ((0, 4), (1, 8)))
    second_gain = jnp.clip(1.0 + 0.18 * jax.random.normal(streams_of[10], (D,), jnp.float32), 0.099609375, 1.8984375).astype(jnp.bfloat16)
    last_gate = centred(streams_of[11], (D, FF), D ** -0.5, 0.125, ((0, 8), (1, 4)))
    last_up = centred(streams_of[12], (D, FF), D ** -0.5, 0.125, ((0, 8), (1, 4)))
    last_down = centred(streams_of[13], (FF, D), FF ** -0.5, 0.078125, ((0, 4), (1, 8)))
    third_gain = jnp.clip(1.0 + 0.18 * jax.random.normal(streams_of[14], (D,), jnp.float32), 0.099609375, 1.8984375).astype(jnp.bfloat16)
    return dict(tokens=tokens, first_gate=first_gate, first_up=first_up, first_down=first_down, first_gain=first_gain, glu_value=glu_value, glu_gate=glu_gate, conv_taps=conv_taps, conv_gain=conv_gain, conv_proj=conv_proj, second_gain=second_gain, last_gate=last_gate, last_up=last_up, last_down=last_down, third_gain=third_gain)


ALPHA = 2.0 ** 0.25
EPSILON = 1e-05

def norm_rows(values, gain):
    center = lax.optimization_barrier(jnp.mean(values, axis=-1, keepdims=True))
    spread = lax.optimization_barrier(jnp.mean(jnp.square(values - center), axis=-1, keepdims=True))
    return (values - center) * lax.rsqrt(spread + EPSILON) * gain.astype(jnp.float32)

def split_sum(hidden, weight):
    blocks = hidden.shape[1] // N_TP
    left = hidden.reshape(hidden.shape[0], N_TP, blocks).astype(jnp.float32)
    right = weight.reshape(N_TP, blocks, weight.shape[1]).astype(jnp.float32)
    parts = jnp.einsum('rbf,bfd->brd', left, right)
    parts = lax.optimization_barrier(parts.astype(jnp.bfloat16))
    return lax.optimization_barrier(jnp.sum(parts.astype(jnp.float32), axis=0))

def feed_forward(current, w_gate, w_up, w_down):
    gate = jnp.dot(current, w_gate, preferred_element_type=jnp.float32)
    upward = jnp.dot(current, w_up, preferred_element_type=jnp.float32)
    hidden = (jax.nn.silu(gate) * upward).astype(jnp.bfloat16)
    return split_sum(hidden, w_down)

def post_norm(current, branch, weight, gain):
    mixed = ALPHA * current.astype(jnp.float32) + weight * branch
    return norm_rows(mixed, gain).astype(jnp.bfloat16)

def conv_module(current, glu_value, glu_gate, conv_taps, conv_gain, conv_proj):
    value = jnp.dot(current, glu_value, preferred_element_type=jnp.float32)
    gate = jnp.dot(current, glu_gate, preferred_element_type=jnp.float32)
    gated = value * jax.nn.sigmoid(gate)
    reach = (conv_taps.shape[0] - 1) // 2
    length = gated.shape[0]
    padded = jnp.pad(gated, ((reach, reach), (0, 0)))
    taps = conv_taps.astype(jnp.float32)
    mixed = jnp.zeros_like(gated)
    for tap_index in range(conv_taps.shape[0]):
        mixed = mixed + taps[tap_index] * padded[tap_index:tap_index + length]
    normed = jax.nn.silu(norm_rows(mixed, conv_gain)).astype(jnp.bfloat16)
    return split_sum(normed, conv_proj)

def reference(tokens, first_gate, first_up, first_down, first_gain, glu_value, glu_gate, conv_taps, conv_gain, conv_proj, second_gain, last_gate, last_up, last_down, third_gain):

    def one_sequence(current):
        first = post_norm(current, feed_forward(current, first_gate, first_up, first_down), 0.5, first_gain)
        second = post_norm(first, conv_module(first, glu_value, glu_gate, conv_taps, conv_gain, conv_proj), 1.0, second_gain)
        return post_norm(second, feed_forward(second, last_gate, last_up, last_down), 0.5, third_gain)
    return lax.map(one_sequence, tokens)
```

```python
import functools

import jax
import jax.numpy as jnp
from jax import lax
from jax.experimental import pallas as pl
from jax.experimental.pallas import tpu as pltpu
from jax.sharding import PartitionSpec as P

ALPHA = 2.0**0.25
EPSILON = 1e-05
MESH = pl.DeviceIdType.MESH
F32 = jnp.float32
BF16 = jnp.bfloat16

CORES = 2
FIRST = (0, 1, 2)
CONV = (3, 4, 5)
LAST = (6, 7, 8)
DOWN = (2, 5, 8)
LEAD = 2


def flip(value, k, size):
    bit = 1
    while bit < size:
        if k & bit:
            value = value + bit - 2 * bit * ((value // bit) % 2)
        bit *= 2
    return value


def layer_kernel(n_z, n_y, n_x, tokens_ref, *refs):
    weights = refs[:9]
    first_gain, conv_taps, conv_gain, second_gain, third_gain = refs[9:14]
    out_ref = refs[14]
    bufs = refs[15:24]
    (xg, xc, hidden, core_out, core_in, side_out, side_in, held, line_out, line_in,
     c_core_out, c_core_in, c_side_out, c_side_in, current, conv_in, acted, stat) = refs[24:42]
    (wz_s, wz_r, wy_s, wy_r, own_s, gz_s, gz_r, gx_s, gx_r, gc_s, gc_r,
     rc_s, rc_r, rx_s, rx_r, rz_s, rz_r, st_s, st_r) = refs[42:]

    n_tp = n_x * CORES
    fs = lax.axis_index("fs")
    tp = lax.axis_index("tp")
    z, y = fs // n_y, fs % n_y
    x, core = tp // CORES, tp % CORES
    length, width = tokens_ref.shape
    features = width * n_tp
    chunk = hidden.shape[2]
    partner = (fs, x * CORES + 1 - core)
    z_order = [flip(z, k, n_z) for k in range(n_z - 1, -1, -1)]

    barrier = pltpu.get_barrier_semaphore()
    for k in range(1, n_z):
        pl.semaphore_signal(barrier, inc=1, device_id=(flip(z, k, n_z) * n_y + y, tp), device_id_type=MESH)
    for o in range(1, n_y):
        pl.semaphore_signal(barrier, inc=1, device_id=(z * n_y + (y + o) % n_y, tp), device_id_type=MESH)
    for o in range(1, n_tp):
        pl.semaphore_signal(barrier, inc=1, device_id=(fs, (tp + o) % n_tp), device_id_type=MESH)
    pl.semaphore_wait(barrier, n_z - 1 + n_y - 1 + n_tp - 1)

    pending = {}

    def remote(src, dst, s, r, dest):
        return pltpu.make_async_remote_copy(
            src_ref=src, dst_ref=dst, send_sem=s, recv_sem=r, device_id=dest, device_id_type=MESH
        )

    def when(ok, fn):
        if ok is None:
            fn()
        else:
            pl.when(ok)(fn)

    def send(group, src, dst, s, r, dest, ok=None):
        when(ok, lambda: remote(src, dst, s, r, dest).start())
        pending.setdefault(group, []).append((ok, lambda: remote(src, dst, s, r, dest).wait_send()))

    def arrive(dst, s, r):
        remote(dst, dst, s, r, (fs, tp)).wait_recv()

    def flush(*groups):
        for group in groups:
            for ok, done in pending.pop(group, []):
                when(ok, done)

    def slot(m, block):
        if m in DOWN:
            return bufs[m].at[block]
        rows = bufs[m].shape[0] // (n_z * n_y)
        return bufs[m].at[pl.ds(pl.multiple_of(block * rows, 16), rows)]

    def part_of(m, zz):
        if m in CONV:
            return weights[m]
        if m in DOWN:
            return weights[m].at[pl.ds(pl.multiple_of(zz * chunk, 16), chunk)]
        if len(weights[m].shape) == 3:
            return weights[m].at[zz]
        return weights[m].at[:, pl.ds(pl.multiple_of(zz * chunk, 128), chunk)]

    def to_y(m, zz, src):
        for o in range(1, n_y):
            send(
                "weights", src, slot(m, zz * n_y + y), wy_s.at[m, zz, o - 1], wy_r.at[m, zz, o - 1],
                (z * n_y + (y + o) % n_y, tp),
            )

    def weight_send(m):
        if m in CONV:
            for side, sign in ((0, 1), (1, -1)):
                ok = z < n_z - 1 if side == 0 else z > 0
                send(
                    "weights", weights[m], slot(m, fs), wz_s.at[m, side], wz_r.at[m, side],
                    (fs + sign * n_y, tp), ok,
                )
        else:
            for k in range(n_z - 1, 0, -1):
                zz = flip(z, k, n_z)
                send("weights", part_of(m, zz), slot(m, fs), wz_s.at[m, k], wz_r.at[m, k], (zz * n_y + y, tp))
        own = part_of(m, z)
        to_y(m, z, own)
        pltpu.make_async_copy(own, slot(m, fs), own_s.at[m]).start()

    def weight_steps(m):
        for k in range(n_z - 1, 0, -1):
            if m in CONV:
                d = n_z - k
                for side, sign in ((0, 1), (1, -1)):
                    zz = z - sign * d
                    here = zz >= 0 if side == 0 else zz < n_z
                    onward = here & (z < n_z - 1 if side == 0 else z > 0)
                    i = (d - 1) * 2 + side
                    block = slot(m, zz * n_y + y)
                    when(here, lambda: arrive(block, wz_s.at[m, i], wz_r.at[m, i]))
                    if d < n_z - 1:
                        send(
                            "weights", block, block, wz_s.at[m, i + 2], wz_r.at[m, i + 2],
                            (fs + sign * n_y, tp), onward,
                        )
                    for o in range(1, n_y):
                        send(
                            "weights", block, block, wy_s.at[m, zz, o - 1], wy_r.at[m, zz, o - 1],
                            (z * n_y + (y + o) % n_y, tp), here,
                        )
            else:
                zz = flip(z, k, n_z)
                block = slot(m, zz * n_y + y)
                arrive(block, wz_s.at[m, k], wz_r.at[m, k])
                to_y(m, zz, block)
            yield

    def weight_ready(m):
        for k in range(n_z):
            zz = flip(z, k, n_z)
            for o in range(1, n_y):
                arrive(slot(m, zz * n_y + (y + n_y - o) % n_y), wy_s.at[m, zz, o - 1], wy_r.at[m, zz, o - 1])
        pltpu.make_async_copy(part_of(m, z), slot(m, fs), own_s.at[m]).wait()

    landed = [0]

    def stream():
        count = len(weights)
        for m in range(LEAD):
            weight_send(m)
        yield
        for m in range(count):
            if m + LEAD < count:
                weight_send(m + LEAD)
            for _ in weight_steps(m):
                yield
            landed[0] = m + 1

    stream_state = stream()

    def pump(steps):
        for _ in range(steps):
            next(stream_state, None)

    def until(*matrices):
        while landed[0] <= max(matrices):
            next(stream_state, None)
        for m in matrices:
            weight_ready(m)

    def columns(t):
        return pl.ds(pl.multiple_of(t * width, 128), width)

    def spread(group, src, dst, x_s, x_r, c_s, c_r, ok=None):
        for o in range(1, n_x):
            send(group, src, dst(tp), x_s(o - 1), x_r(o - 1), (fs, (x + o) % n_x * CORES + core), ok)
        send(group, src, dst(tp), c_s(x), c_r(x), partner, ok)

    def pass_on(group, dst, x_s, x_r, c_s, c_r, ok=None):
        for o in range(1, n_x):
            xx = (x + n_x - o) % n_x
            block = dst(xx * CORES + core)
            when(ok, lambda: arrive(block, x_s(o - 1), x_r(o - 1)))
            send(group, block, block, c_s(xx), c_r(xx), partner, ok)

    def collect(dst, c_s, c_r, ok=None):
        for o in range(n_x):
            xx = (x + o) % n_x
            when(ok, lambda: arrive(dst(xx * CORES + 1 - core), c_s(xx), c_r(xx)))

    def seq_refs(f, zz):
        return (
            lambda t: xg.at[f, zz, :, columns(t)],
            lambda i: gx_s.at[f, zz, i], lambda i: gx_r.at[f, zz, i],
            lambda i: gc_s.at[f, zz, i], lambda i: gc_r.at[f, zz, i],
        )

    def sides(d):
        for side, sign in ((0, 1), (1, -1)):
            zz = z - sign * d
            yield side, sign, zz, (zz >= 0 if side == 0 else zz < n_z)

    def gather(f, src, use=None):
        group = ("gather", f)
        for side, sign in ((0, 1), (1, -1)):
            ok = z < n_z - 1 if side == 0 else z > 0
            send(
                group, src, xg.at[f, z, :, columns(tp)], gz_s.at[f, side], gz_r.at[f, side],
                (fs + sign * n_y, tp), ok,
            )
        spread(group, src, *seq_refs(f, z))
        xg[f, z, :, columns(tp)] = src[...]
        yield
        for d in range(1, n_z + 1):
            if d < n_z:
                for side, sign, zz, here in sides(d):
                    onward = here & (z < n_z - 1 if side == 0 else z > 0)
                    i = (d - 1) * 2 + side
                    block = xg.at[f, zz, :, columns(tp)]
                    when(here, lambda: arrive(block, gz_s.at[f, i], gz_r.at[f, i]))
                    if d < n_z - 1:
                        send(
                            group, block, block, gz_s.at[f, i + 2], gz_r.at[f, i + 2],
                            (fs + sign * n_y, tp), onward,
                        )
                    spread(group, block, *seq_refs(f, zz), ok=here)
            yield
            if d == 1:
                pass_on(group, *seq_refs(f, z))
            else:
                for side, sign, zz, here in sides(d - 1):
                    pass_on(group, *seq_refs(f, zz), ok=here)
            yield
            if d == 1:
                dst, _, _, c_s, c_r = seq_refs(f, z)
                collect(dst, c_s, c_r)
                if use is not None:
                    use(z, None)
            else:
                for side, sign, zz, here in sides(d - 1):
                    dst, _, _, c_s, c_r = seq_refs(f, zz)
                    collect(dst, c_s, c_r, here)
                    if use is not None:
                        use(zz, here)

    def ffn_hidden(f, zz, gate, up):
        rows = xg[f, zz]
        g = jnp.dot(rows, gate[...], preferred_element_type=F32)
        u = jnp.dot(rows, up[...], preferred_element_type=F32)
        hidden[zz] = (g * jax.nn.sigmoid(g) * u).astype(BF16)

    def project(source, down, t):
        part = down.shape[2]
        per = width // part
        for q in range(per):
            yield slice(q * part, (q + 1) * part), jnp.dot(source[...], down[t * per + q], preferred_element_type=F32)

    def reduce_give(group, source, down, outgoing, incoming, s, r):
        for o in [*range(1, n_x), 0]:
            xx = (x + o) % n_x
            for cols, value in project(source, down, xx * CORES + 1 - core):
                outgoing(xx)[:, cols] = value.astype(BF16)
            send(group, outgoing(xx), incoming(xx), s(xx), r(xx), partner)

    def reduce_take(group, source, down, incoming, s, r, outgoing, target, xs, xr, keep):
        for o in [*range(1, n_x), 0]:
            xx = (x + o) % n_x
            arrive(incoming(xx), s(xx), r(xx))
            for cols, value in project(source, down, xx * CORES + core):
                total = value + incoming(xx)[:, cols].astype(F32)
                if o:
                    outgoing(o - 1)[:, cols] = total.astype(BF16)
                else:
                    keep[:, cols] = total
            if o:
                send(group, outgoing(o - 1), target(o - 1), xs(o - 1), xr(o - 1), (fs, xx * CORES + core))

    def reduce_sum(target, xs, xr, keep):
        total = keep[...]
        for o in range(1, n_x):
            arrive(target(o - 1), xs(o - 1), xr(o - 1))
            total = total + target(o - 1)[...].astype(F32)
        keep[...] = total

    def reduce_ffn(f, down, pumps):
        group = ("reduce", f)

        def give(zz):
            reduce_give(
                group, hidden.at[zz], down, lambda i: core_out.at[zz, i], lambda i: core_in.at[zz, i],
                lambda i: rc_s.at[f, zz, i], lambda i: rc_r.at[f, zz, i],
            )

        def take(zz):
            reduce_take(
                group, hidden.at[zz], down, lambda i: core_in.at[zz, i],
                lambda i: rc_s.at[f, zz, i], lambda i: rc_r.at[f, zz, i],
                lambda i: side_out.at[zz, i], lambda i: side_in.at[zz, i],
                lambda i: rx_s.at[f, zz, i], lambda i: rx_r.at[f, zz, i], held.at[zz],
            )

        give(z_order[0])
        for i in range(n_z):
            if i + 1 < n_z:
                give(z_order[i + 1])
            take(z_order[i])
        for i, zz in enumerate(z_order):
            pump(pumps)
            reduce_sum(
                lambda j: side_in.at[zz, j], lambda j: rx_s.at[f, zz, j], lambda j: rx_r.at[f, zz, j], held.at[zz]
            )
            own = i == n_z - 1
            for side, there in ((0, z > 0), (1, z < n_z - 1)):
                if not own:
                    there = there & (zz > z if side == 0 else zz < z)

                def add(side=side):
                    arrive(line_in.at[side, zz], rz_s.at[f, side, zz], rz_r.at[f, side, zz])
                    held[zz] = held[zz] + line_in[side, zz].astype(F32)

                when(there, add)
            if not own:
                line_out[zz] = held[zz].astype(BF16)
                for side, sign in ((0, 1), (1, -1)):
                    send(
                        group, line_out.at[zz], line_in.at[side, zz], rz_s.at[f, side, zz], rz_r.at[f, side, zz],
                        (fs + sign * n_y, tp), zz > z if side == 0 else zz < z,
                    )
        return held[z]

    def stats_start(phase, values):
        sums = jnp.sum(values, axis=-1, keepdims=True)
        squares = jnp.sum(values * values, axis=-1, keepdims=True)
        lane = lax.broadcasted_iota(jnp.int32, (values.shape[0], 128), 1)
        both = jnp.where(lane == 0, sums, jnp.where(lane == 1, squares, 0.0))
        stat[phase, n_tp - 1] = both.T[:8]
        for step in range(1, n_tp):
            i = step - 1
            remote(
                stat.at[phase, n_tp - 1], stat.at[phase, i], st_s.at[phase, i], st_r.at[phase, i],
                (fs, (tp + step) % n_tp),
            ).start()

    def stats_wait(phase, all_width):
        for step in range(1, n_tp):
            i = step - 1
            remote(
                stat.at[phase, n_tp - 1], stat.at[phase, i], st_s.at[phase, i], st_r.at[phase, i], (fs, tp)
            ).wait()
        total = stat[phase, 0]
        for i in range(1, n_tp):
            total = total + stat[phase, i]
        both = jnp.concatenate([total] * 16, axis=0).T
        center = both[:, 0:1] / all_width
        spread_of = both[:, 1:2] / all_width - center * center
        return center, lax.rsqrt(spread_of + EPSILON)

    def post_norm(phase, gain):
        stats_start(phase, current[...])
        pump(1)
        center, scale = stats_wait(phase, features)
        return ((current[...] - center) * scale * gain[...].astype(F32)).astype(BF16)

    steps = gather(0, tokens_ref)
    next(steps)
    pump(1)
    for _ in steps:
        pump(1)
    until(0, 1)
    lax.fori_loop(0, n_z, lambda i, c: (ffn_hidden(0, i, bufs[0], bufs[1]), c)[1], 0)
    until(2)
    current[...] = ALPHA * tokens_ref[...].astype(F32) + 0.5 * reduce_ffn(0, bufs[2], 1)
    first = post_norm(0, first_gain)
    out_ref[...] = first

    conv_refs = (
        lambda t: xc.at[:, columns(t)],
        lambda i: gx_s.at[2, 0, i], lambda i: gx_r.at[2, 0, i],
        lambda i: gc_s.at[2, 0, i], lambda i: gc_r.at[2, 0, i],
    )
    spread("conv", out_ref, *conv_refs)
    xc[:, columns(tp)] = first
    until(3, 4)
    pass_on("conv", *conv_refs)
    collect(conv_refs[0], conv_refs[3], conv_refs[4])

    channels = acted.shape[1]
    taps = conv_taps.shape[0]
    reach = (taps - 1) // 2
    margin = (conv_in.shape[0] - length) // 2
    rows = xc[...]
    value = jnp.dot(rows, bufs[3][...], preferred_element_type=F32)
    gate = jnp.dot(rows, bufs[4][...], preferred_element_type=F32)
    conv_in[0:margin] = jnp.zeros((margin, channels), F32)
    conv_in[margin + length :] = jnp.zeros((margin, channels), F32)
    conv_in[margin : margin + length] = value * jax.nn.sigmoid(gate)
    pump(1)
    rows_each = length // 4
    for low in range(0, length, rows_each):
        for left in range(0, channels, 128):
            cols = slice(left, left + 128)
            total = jnp.zeros((rows_each, 128), F32)
            for tap in range(taps):
                start = margin - reach + low + tap
                total = total + conv_taps[tap : tap + 1, cols].astype(F32) * conv_in[start : start + rows_each, cols]
            current[low : low + rows_each, cols] = total
    stats_start(1, current[:, 0:channels])
    pump(1)
    center, scale = stats_wait(1, channels * n_tp)
    normed = (current[:, 0:channels] - center) * scale * conv_gain[...].astype(F32)
    acted[...] = (normed * jax.nn.sigmoid(normed)).astype(BF16)
    until(5)
    conv_core = (
        lambda i: rc_s.at[2, 0, i], lambda i: rc_r.at[2, 0, i],
    )
    conv_side = (lambda i: rx_s.at[2, 0, i], lambda i: rx_r.at[2, 0, i])
    reduce_give("conv", acted, bufs[5], lambda i: c_core_out.at[i], lambda i: c_core_in.at[i], *conv_core)
    pump(1)
    reduce_take(
        "conv", acted, bufs[5], lambda i: c_core_in.at[i], *conv_core,
        lambda i: c_side_out.at[i], lambda i: c_side_in.at[i], *conv_side, current,
    )
    pump(2)
    reduce_sum(lambda i: c_side_in.at[i], *conv_side, current)
    current[...] = ALPHA * out_ref[...].astype(F32) + current[...]
    second = post_norm(2, second_gain)
    flush("conv")
    out_ref[...] = second

    steps = gather(1, out_ref)
    next(steps)
    until(6, 7)
    for _ in steps:
        pump(1)
    lax.fori_loop(0, n_z, lambda i, c: (ffn_hidden(1, i, bufs[6], bufs[7]), c)[1], 0)
    until(8)
    flush(("reduce", 0))
    current[...] = ALPHA * out_ref[...].astype(F32) + 0.5 * reduce_ffn(1, bufs[8], 1)
    pump(100)
    normed = post_norm(3, third_gain)
    flush("weights", ("gather", 0), ("gather", 1), ("reduce", 1))
    out_ref[...] = normed


def solution(mesh):
    n_fs, n_tp = mesh.shape["fs"], mesh.shape["tp"]
    n_y = 1 << ((n_fs.bit_length() - 1) // 2)
    n_z, n_x = n_fs // n_y, n_tp // CORES

    def body(
        tokens, first_gate, first_up, first_down, first_gain, glu_value, glu_gate, conv_taps, conv_gain,
        conv_proj, second_gain, last_gate, last_up, last_down, third_gain,
    ):
        tokens = tokens[0]
        length, width = tokens.shape
        features = width * n_tp
        chunk = first_gate.shape[1] // n_z

        def by_chunk(w):
            if chunk % 128 == 0:
                return w
            return jnp.swapaxes(w.reshape(w.shape[0], n_z, chunk), 0, 1)

        weights = (
            by_chunk(first_gate), by_chunk(first_up), first_down, glu_value, glu_gate, conv_proj,
            by_chunk(last_gate), by_chunk(last_up), last_down,
        )
        channels = glu_value.shape[1]
        reach = (conv_taps.shape[0] - 1) // 2
        margin = -(-reach // 8) * 8
        part = first_down.shape[1]
        wide = pltpu.VMEM((features, chunk), BF16)
        down = pltpu.VMEM((n_fs, chunk, part), BF16)
        glu = pltpu.VMEM((features, channels), BF16)
        proj = pltpu.VMEM((n_fs, channels, part), BF16)
        dma = pltpu.SemaphoreType.DMA
        vmem = pl.BlockSpec(memory_space=pltpu.VMEM)
        others = max(n_x - 1, 1)

        def blocks(*lead, kind=BF16):
            return pltpu.VMEM(lead + (length, width), kind)

        def pair(*shape):
            return [dma(shape), dma(shape)]

        result = pl.pallas_call(
            functools.partial(layer_kernel, n_z, n_y, n_x),
            out_shape=jax.ShapeDtypeStruct((length, width), BF16),
            in_specs=[vmem] + [pl.BlockSpec(memory_space=pl.ANY)] * 9 + [vmem] * 5,
            out_specs=vmem,
            scratch_shapes=[wide, wide, down, glu, glu, proj, wide, wide, down]
            + [
                pltpu.VMEM((2, n_z, length, features), BF16),
                pltpu.VMEM((length, features), BF16),
                pltpu.VMEM((n_z, length, chunk), BF16),
                blocks(n_z, n_x),
                blocks(n_z, n_x),
                blocks(n_z, others),
                blocks(n_z, others),
                blocks(n_z, kind=F32),
                blocks(n_z),
                blocks(2, n_z),
                blocks(n_x),
                blocks(n_x),
                blocks(others),
                blocks(others),
                blocks(kind=F32),
                pltpu.VMEM((length + 2 * margin, channels), F32),
                pltpu.VMEM((length, channels), BF16),
                pltpu.VMEM((4, n_tp, 8, length), F32),
            ]
            + pair(9, 2 * n_z)
            + pair(9, n_z, max(n_y - 1, 1))
            + [dma((9,))]
            + pair(2, 2 * n_z)
            + pair(3, n_z, others)
            + pair(3, n_z, n_x)
            + pair(3, n_z, n_x)
            + pair(3, n_z, others)
            + pair(2, 2, n_z)
            + pair(4, n_tp - 1),
            compiler_params=pltpu.CompilerParams(
                collective_id=0, has_side_effects=True, vmem_limit_bytes=67000000
            ),
        )(
            tokens, *weights, first_gain[None], conv_taps, conv_gain[None], second_gain[None], third_gain[None]
        )
        return result[None]

    weight = P("fs", "tp")
    return jax.shard_map(
        body,
        mesh=mesh,
        in_specs=(
            P("fs", None, "tp"), weight, weight, P("tp", "fs"), P("tp"), weight, weight, P(None, "tp"), P("tp"),
            P("tp", "fs"), P("tp"), weight, weight, P("tp", "fs"), P("tp"),
        ),
        out_specs=P("fs", None, "tp"),
        check_vma=False,
    )
```

```python
import functools

import jax
import jax.numpy as jnp
from jax import lax
from jax.experimental import pallas as pl
from jax.experimental.pallas import tpu as pltpu
from jax.sharding import PartitionSpec as P

ALPHA = 2.0**0.25
EPSILON = 1e-05
MESH = pl.DeviceIdType.MESH
F32 = jnp.float32
BF16 = jnp.bfloat16

CORES = 2
FIRST = (0, 1, 2)
CONV = (3, 4, 5)
LAST = (6, 7, 8)
DOWN = (2, 5, 8)


def flip(value, k, size):
    bit = 1
    while bit < size:
        if k & bit:
            value = value + bit - 2 * bit * ((value // bit) % 2)
        bit *= 2
    return value


def low(k):
    return k & -k


def bits_below(limit):
    bit = 1
    while bit < limit:
        yield bit
        bit *= 2


def layer_kernel(n_z, n_y, n_x, cuts, tokens_ref, *refs):
    weights = refs[:9]
    first_gain, conv_taps, conv_gain, second_gain, third_gain = refs[9:14]
    out_ref = refs[14]
    bufs = refs[15:24]
    xgs, hiddens = refs[24:26], refs[26:28]
    (xc, core_out, core_in, side_out, side_in, held, line_out, line_in,
     c_core_out, c_core_in, c_side_out, c_side_in, current, conv_in, acted, stat) = refs[28:44]
    (wz_s, wz_r, wy_s, wy_r, own_s, gz_s, gz_r, gx_s, gx_r, gc_s, gc_r,
     rc_s, rc_r, rx_s, rx_r, rz_s, rz_r, st_s, st_r) = refs[44:]

    n_tp = n_x * CORES
    fs = lax.axis_index("fs")
    tp = lax.axis_index("tp")
    z, y = fs // n_y, fs % n_y
    x, core = tp // CORES, tp % CORES
    length, width = tokens_ref.shape
    features = width * n_tp
    partner = (fs, x * CORES + 1 - core)

    def along(k):
        return (flip(z, k, n_z) * n_y + y, tp)


    barrier = pltpu.get_barrier_semaphore()
    for k in range(1, n_z):
        pl.semaphore_signal(barrier, inc=1, device_id=(flip(z, k, n_z) * n_y + y, tp), device_id_type=MESH)
    for o in range(1, n_y):
        pl.semaphore_signal(barrier, inc=1, device_id=(z * n_y + (y + o) % n_y, tp), device_id_type=MESH)
    for o in range(1, n_tp):
        pl.semaphore_signal(barrier, inc=1, device_id=(fs, (tp + o) % n_tp), device_id_type=MESH)
    pl.semaphore_wait(barrier, n_z - 1 + n_y - 1 + n_tp - 1)

    pending = {}

    def remote(src, dst, s, r, dest):
        return pltpu.make_async_remote_copy(
            src_ref=src, dst_ref=dst, send_sem=s, recv_sem=r, device_id=dest, device_id_type=MESH
        )

    def send(group, src, dst, s, r, dest):
        copy = remote(src, dst, s, r, dest)
        copy.start()
        pending.setdefault(group, []).append(copy)

    def arrive(dst, s, r):
        remote(dst, dst, s, r, (fs, tp)).wait_recv()

    def flush(*groups):
        for group in groups:
            for copy in pending.pop(group, []):
                copy.wait_send()

    def slot(m, block):
        if m in DOWN:
            return bufs[m].at[block]
        rows = bufs[m].shape[0] // (n_z * n_y)
        return bufs[m].at[pl.ds(pl.multiple_of(block * rows, 16), rows)]

    def part_of(m, zz):
        if m in CONV:
            return weights[m]
        place = zz % cuts[m in LAST]
        chunk = hiddens[m in LAST].shape[2]
        if m in DOWN:
            return weights[m].at[pl.ds(pl.multiple_of(place * chunk, 16), chunk)]
        if len(weights[m].shape) == 3:
            return weights[m].at[place]
        return weights[m].at[:, pl.ds(pl.multiple_of(place * chunk, 128), chunk)]

    def to_y(m, k, src):
        for o in range(1, n_y):
            send(
                "weights", src, slot(m, along(k)[0]), wy_s.at[m, k, o - 1], wy_r.at[m, k, o - 1],
                (z * n_y + (y + o) % n_y, tp),
            )

    def tree_send(group, k, src, dst, s, r):
        for bit in bits_below(low(k) if k else n_z):
            send(group, src, dst, s(k ^ bit), r(k ^ bit), along(bit))

    def weight_own(*matrices):
        for m in matrices:
            own = part_of(m, z)
            to_y(m, 0, own)
            pltpu.make_async_copy(own, slot(m, fs), own_s.at[m]).start()

    def unit_send(m, k):
        zz = flip(z, k, n_z)
        send("weights", part_of(m, zz), slot(m, fs), wz_s.at[m, k], wz_r.at[m, k], along(k))

    def unit_forward(m, k):
        block = slot(m, along(k)[0])
        arrive(block, wz_s.at[m, k], wz_r.at[m, k])
        to_y(m, k, block)

    def conv_start():
        for m in CONV:
            tree_send("weights", 0, weights[m], slot(m, fs), lambda k: wz_s.at[m, k], lambda k: wz_r.at[m, k])
        weight_own(*CONV)

    def conv_block(k):
        for m in CONV:
            block = slot(m, along(k)[0])
            arrive(block, wz_s.at[m, k], wz_r.at[m, k])
            tree_send("weights", k, block, block, lambda i: wz_s.at[m, i], lambda i: wz_r.at[m, i])
            to_y(m, k, block)

    def weight_ready(m):
        for k in range(n_z):
            zz = flip(z, k, n_z)
            for o in range(1, n_y):
                arrive(slot(m, zz * n_y + (y + n_y - o) % n_y), wy_s.at[m, k, o - 1], wy_r.at[m, k, o - 1])
        pltpu.make_async_copy(part_of(m, z), slot(m, fs), own_s.at[m]).wait()

    units = [(m, k) for m in FIRST + LAST for k in range(n_z - 1, 0, -1)]
    sent, landed = [0], [0]

    def issue(count):
        for unit in units[sent[0] : sent[0] + count]:
            unit_send(*unit)
        sent[0] = min(sent[0] + count, len(units))

    def forward(count):
        for unit in units[landed[0] : landed[0] + count]:
            unit_forward(*unit)
        landed[0] = min(landed[0] + count, len(units))

    def until(*matrices):
        need = 1 + max((n for n, unit in enumerate(units) if unit[0] in matrices), default=-1)
        issue(max(need - sent[0], 0))
        forward(max(need - landed[0], 0))
        for m in matrices:
            weight_ready(m)

    def act(step):
        for fn, *args in step:
            fn(*args)

    def columns(t):
        return pl.ds(pl.multiple_of(t * width, 128), width)

    def spread(group, src, dst, x_s, x_r, c_s, c_r):
        for o in range(1, n_x):
            send(group, src, dst(tp), x_s(o - 1), x_r(o - 1), (fs, (x + o) % n_x * CORES + core))
        send(group, src, dst(tp), c_s(x), c_r(x), partner)

    def pass_on(group, dst, x_s, x_r, c_s, c_r):
        for o in range(1, n_x):
            xx = (x + n_x - o) % n_x
            block = dst(xx * CORES + core)
            arrive(block, x_s(o - 1), x_r(o - 1))
            send(group, block, block, c_s(xx), c_r(xx), partner)

    def collect(dst, x_s, x_r, c_s, c_r):
        for o in range(n_x):
            xx = (x + o) % n_x
            arrive(dst(xx * CORES + 1 - core), c_s(xx), c_r(xx))

    def seq_refs(f, k):
        return (
            lambda t: xgs[f].at[k, :, columns(t)],
            lambda i: gx_s.at[f, k, i], lambda i: gx_r.at[f, k, i],
            lambda i: gc_s.at[f, k, i], lambda i: gc_r.at[f, k, i],
        )

    def gather_start(f, src):
        group = ("gather", f)
        for bit in bits_below(cuts[f]):
            send(group, src, xgs[f].at[bit, :, columns(tp)], gz_s.at[f, bit], gz_r.at[f, bit], along(bit))
        spread(group, src, *seq_refs(f, 0))
        xgs[f][0, :, columns(tp)] = src[...]

    def gather_block(f, k):
        group = ("gather", f)
        block = xgs[f].at[k, :, columns(tp)]
        arrive(block, gz_s.at[f, k], gz_r.at[f, k])
        for bit in bits_below(low(k)):
            send(group, block, xgs[f].at[k ^ bit, :, columns(tp)], gz_s.at[f, k ^ bit], gz_r.at[f, k ^ bit], along(bit))
        spread(group, block, *seq_refs(f, k))

    def gather_pass(f, k):
        pass_on(("gather", f), *seq_refs(f, k))

    def ffn_hidden(f, k, gate, up):
        rows = xgs[f][k]
        g = jnp.dot(rows, gate[...], preferred_element_type=F32)
        u = jnp.dot(rows, up[...], preferred_element_type=F32)
        hiddens[f][k] = (g * jax.nn.sigmoid(g) * u).astype(BF16)

    def project(source, down, t):
        part = down.shape[2]
        per = width // part
        for q in range(per):
            yield slice(q * part, (q + 1) * part), jnp.dot(source[...], down[t * per + q], preferred_element_type=F32)

    def reduce_give(group, source, down, outgoing, incoming, s, r):
        for o in [*range(1, n_x), 0]:
            xx = (x + o) % n_x
            for cols, value in project(source, down, xx * CORES + 1 - core):
                outgoing(xx)[:, cols] = value.astype(BF16)
            send(group, outgoing(xx), incoming(xx), s(xx), r(xx), partner)

    def reduce_take(group, source, down, incoming, s, r, outgoing, target, xs, xr, keep):
        for o in [*range(1, n_x), 0]:
            xx = (x + o) % n_x
            arrive(incoming(xx), s(xx), r(xx))
            for cols, value in project(source, down, xx * CORES + core):
                total = value + incoming(xx)[:, cols].astype(F32)
                if o:
                    outgoing(o - 1)[:, cols] = total.astype(BF16)
                else:
                    keep[:, cols] = total
            if o:
                send(group, outgoing(o - 1), target(o - 1), xs(o - 1), xr(o - 1), (fs, xx * CORES + core))

    def reduce_sum(target, xs, xr, keep):
        total = keep[...]
        for o in range(1, n_x):
            arrive(target(o - 1), xs(o - 1), xr(o - 1))
            total = total + target(o - 1)[...].astype(F32)
        keep[...] = total

    def reduce_ffn(f, down, plan):
        group = ("reduce", f)

        def give(k):
            reduce_give(
                group, hiddens[f].at[k], down, lambda i: core_out.at[k, i], lambda i: core_in.at[k, i],
                lambda i: rc_s.at[f, k, i], lambda i: rc_r.at[f, k, i],
            )

        def take(k):
            reduce_take(
                group, hiddens[f].at[k], down, lambda i: core_in.at[k, i],
                lambda i: rc_s.at[f, k, i], lambda i: rc_r.at[f, k, i],
                lambda i: side_out.at[k, i], lambda i: side_in.at[k, i],
                lambda i: rx_s.at[f, k, i], lambda i: rx_r.at[f, k, i], held.at[k],
            )

        give(cuts[f] - 1)
        for k in range(cuts[f] - 1, -1, -1):
            if k:
                give(k - 1)
            take(k)
        act(plan.get("given", ()))
        for k in range(cuts[f] - 1, -1, -1):
            act(plan.get(k, ()))
            reduce_sum(
                lambda i: side_in.at[k, i], lambda i: rx_s.at[f, k, i], lambda i: rx_r.at[f, k, i], held.at[k]
            )
            total = held[k]
            for bit in bits_below(low(k) if k else cuts[f]):
                i = (k ^ bit) - 1
                arrive(line_in.at[i], rz_s.at[f, i], rz_r.at[f, i])
                total = total + line_in[i].astype(F32)
            if k == 0:
                return total
            line_out[k - 1] = total.astype(BF16)
            send(group, line_out.at[k - 1], line_in.at[k - 1], rz_s.at[f, k - 1], rz_r.at[f, k - 1], along(low(k)))

    def stats_start(phase, values):
        sums = jnp.sum(values, axis=-1, keepdims=True)
        squares = jnp.sum(values * values, axis=-1, keepdims=True)
        lane = lax.broadcasted_iota(jnp.int32, (values.shape[0], 128), 1)
        both = jnp.where(lane == 0, sums, jnp.where(lane == 1, squares, 0.0))
        stat[phase, n_tp - 1] = both.T[:8]
        for step in range(1, n_tp):
            i = step - 1
            remote(
                stat.at[phase, n_tp - 1], stat.at[phase, i], st_s.at[phase, i], st_r.at[phase, i],
                (fs, (tp + step) % n_tp),
            ).start()

    def stats_wait(phase, all_width):
        for step in range(1, n_tp):
            i = step - 1
            remote(
                stat.at[phase, n_tp - 1], stat.at[phase, i], st_s.at[phase, i], st_r.at[phase, i], (fs, tp)
            ).wait()
        total = stat[phase, 0]
        for i in range(1, n_tp):
            total = total + stat[phase, i]
        both = jnp.concatenate([total] * 16, axis=0).T
        center = both[:, 0:1] / all_width
        spread_of = both[:, 1:2] / all_width - center * center
        return center, lax.rsqrt(spread_of + EPSILON)

    def post_norm(phase, gain):
        stats_start(phase, current[...])
        center, scale = stats_wait(phase, features)
        return ((current[...] - center) * scale * gain[...].astype(F32)).astype(BF16)

    gather_start(0, tokens_ref)
    weight_own(*FIRST)
    issue(3)
    gather_block(0, 1)
    issue(1)
    gather_block(0, 2)
    issue(2)
    gather_pass(0, 0)
    forward(2)
    gather_block(0, 3)
    issue(3)
    conv_start()
    issue(1)
    gather_pass(0, 1)
    forward(1)
    gather_pass(0, 2)
    forward(1)
    gather_pass(0, 3)
    for k in range(n_z):
        collect(*seq_refs(0, k))
    until(0, 1)
    lax.fori_loop(0, n_z, lambda i, c: (ffn_hidden(0, i, bufs[0], bufs[1]), c)[1], 0)
    until(2)
    weight_own(LAST[0])
    current[...] = ALPHA * tokens_ref[...].astype(F32) + 0.5 * reduce_ffn(0, bufs[2], {
        "given": [(conv_block, 1), (conv_block, 2), (issue, 1)],
        2: [(forward, 1), (issue, 1)],
        1: [(forward, 1), (weight_own, LAST[1]), (issue, 1)],
        0: [(weight_own, LAST[2]), (issue, 1)],
    })
    first = post_norm(0, first_gain)
    out_ref[...] = first

    conv_refs = (
        lambda t: xc.at[:, columns(t)],
        lambda i: gx_s.at[2, 0, i], lambda i: gx_r.at[2, 0, i],
        lambda i: gc_s.at[2, 0, i], lambda i: gc_r.at[2, 0, i],
    )
    spread("conv", out_ref, *conv_refs)
    issue(1)
    xc[:, columns(tp)] = first
    conv_block(3)
    forward(2)
    pass_on("conv", *conv_refs)
    until(3, 4)
    collect(*conv_refs)

    channels = acted.shape[1]
    taps = conv_taps.shape[0]
    reach = (taps - 1) // 2
    margin = (conv_in.shape[0] - length) // 2
    rows = xc[...]
    value = jnp.dot(rows, bufs[3][...], preferred_element_type=F32)
    gate = jnp.dot(rows, bufs[4][...], preferred_element_type=F32)
    conv_in[0:margin] = jnp.zeros((margin, channels), F32)
    conv_in[margin + length :] = jnp.zeros((margin, channels), F32)
    conv_in[margin : margin + length] = value * jax.nn.sigmoid(gate)
    issue(2)
    forward(1)
    rows_each = length // 4
    for top in range(0, length, rows_each):
        for left in range(0, channels, 128):
            cols = slice(left, left + 128)
            total = jnp.zeros((rows_each, 128), F32)
            for tap in range(taps):
                start = margin - reach + top + tap
                total = total + conv_taps[tap : tap + 1, cols].astype(F32) * conv_in[start : start + rows_each, cols]
            current[top : top + rows_each, cols] = total
    stats_start(1, current[:, 0:channels])
    center, scale = stats_wait(1, channels * n_tp)
    normed = (current[:, 0:channels] - center) * scale * conv_gain[...].astype(F32)
    acted[...] = (normed * jax.nn.sigmoid(normed)).astype(BF16)
    until(5)
    conv_core = (lambda i: rc_s.at[2, 0, i], lambda i: rc_r.at[2, 0, i])
    conv_side = (lambda i: rx_s.at[2, 0, i], lambda i: rx_r.at[2, 0, i])
    reduce_give("conv", acted, bufs[5], lambda i: c_core_out.at[i], lambda i: c_core_in.at[i], *conv_core)
    issue(1)
    forward(1)
    reduce_take(
        "conv", acted, bufs[5], lambda i: c_core_in.at[i], *conv_core,
        lambda i: c_side_out.at[i], lambda i: c_side_in.at[i], *conv_side, current,
    )
    forward(1)
    reduce_sum(lambda i: c_side_in.at[i], *conv_side, current)
    current[...] = ALPHA * out_ref[...].astype(F32) + current[...]
    second = post_norm(2, second_gain)
    flush("conv")
    out_ref[...] = second

    gather_start(1, out_ref)
    forward(1)
    gather_block(1, 1)
    forward(1)
    gather_pass(1, 0)
    until(6, 7)
    collect(*seq_refs(1, 0))
    ffn_hidden(1, 0, bufs[6], bufs[7])
    for k in range(1, cuts[1]):
        if k > 1:
            gather_block(1, k)
        gather_pass(1, k)
        collect(*seq_refs(1, k))
        ffn_hidden(1, k, bufs[6], bufs[7])
    until(8)
    flush(("reduce", 0))
    current[...] = ALPHA * out_ref[...].astype(F32) + 0.5 * reduce_ffn(1, bufs[8], {})
    normed = post_norm(3, third_gain)
    flush("weights", ("gather", 0), ("gather", 1), ("reduce", 1))
    out_ref[...] = normed


def solution(mesh):
    n_fs, n_tp = mesh.shape["fs"], mesh.shape["tp"]
    n_y = 1 << ((n_fs.bit_length() - 1) // 2)
    n_z, n_x = n_fs // n_y, n_tp // CORES

    def body(
        tokens, first_gate, first_up, first_down, first_gain, glu_value, glu_gate, conv_taps, conv_gain,
        conv_proj, second_gain, last_gate, last_up, last_down, third_gain,
    ):
        tokens = tokens[0]
        length, width = tokens.shape
        features = width * n_tp
        cuts = (n_z, min(n_z, 2))
        chunks = [first_gate.shape[1] // cut for cut in cuts]

        def by_chunk(w, f):
            if chunks[f] % 128 == 0:
                return w
            return jnp.swapaxes(w.reshape(w.shape[0], cuts[f], chunks[f]), 0, 1)

        weights = (
            by_chunk(first_gate, 0), by_chunk(first_up, 0), first_down, glu_value, glu_gate, conv_proj,
            by_chunk(last_gate, 1), by_chunk(last_up, 1), last_down,
        )
        channels = glu_value.shape[1]
        reach = (conv_taps.shape[0] - 1) // 2
        margin = -(-reach // 8) * 8
        part = first_down.shape[1]
        wide = [pltpu.VMEM((features, chunk), BF16) for chunk in chunks]
        down = [pltpu.VMEM((n_fs, chunk, part), BF16) for chunk in chunks]
        glu = pltpu.VMEM((features, channels), BF16)
        proj = pltpu.VMEM((n_fs, channels, part), BF16)
        dma = pltpu.SemaphoreType.DMA
        vmem = pl.BlockSpec(memory_space=pltpu.VMEM)
        others, others_z = max(n_x - 1, 1), max(n_z - 1, 1)

        def blocks(*lead, kind=BF16):
            return pltpu.VMEM(lead + (length, width), kind)

        def pair(*shape):
            return [dma(shape), dma(shape)]

        result = pl.pallas_call(
            functools.partial(layer_kernel, n_z, n_y, n_x, cuts),
            out_shape=jax.ShapeDtypeStruct((length, width), BF16),
            in_specs=[vmem] + [pl.BlockSpec(memory_space=pl.ANY)] * 9 + [vmem] * 5,
            out_specs=vmem,
            scratch_shapes=[wide[0], wide[0], down[0], glu, glu, proj, wide[1], wide[1], down[1]]
            + [pltpu.VMEM((cut, length, features), BF16) for cut in cuts]
            + [pltpu.VMEM((cut, length, chunk), BF16) for cut, chunk in zip(cuts, chunks)]
            + [
                pltpu.VMEM((length, features), BF16),
                blocks(n_z, n_x),
                blocks(n_z, n_x),
                blocks(n_z, others),
                blocks(n_z, others),
                blocks(n_z, kind=F32),
                blocks(others_z),
                blocks(others_z),
                blocks(n_x),
                blocks(n_x),
                blocks(others),
                blocks(others),
                blocks(kind=F32),
                pltpu.VMEM((length + 2 * margin, channels), F32),
                pltpu.VMEM((length, channels), BF16),
                pltpu.VMEM((4, n_tp, 8, length), F32),
            ]
            + pair(9, n_z)
            + pair(9, n_z, max(n_y - 1, 1))
            + [dma((9,))]
            + pair(2, n_z)
            + pair(3, n_z, others)
            + pair(3, n_z, n_x)
            + pair(3, n_z, n_x)
            + pair(3, n_z, others)
            + pair(2, others_z)
            + pair(4, n_tp - 1),
            compiler_params=pltpu.CompilerParams(
                collective_id=0, has_side_effects=True, vmem_limit_bytes=67000000
            ),
        )(
            tokens, *weights, first_gain[None], conv_taps, conv_gain[None], second_gain[None], third_gain[None]
        )
        return result[None]

    weight = P("fs", "tp")
    return jax.shard_map(
        body,
        mesh=mesh,
        in_specs=(
            P("fs", None, "tp"), weight, weight, P("tp", "fs"), P("tp"), weight, weight, P(None, "tp"), P("tp"),
            P("tp", "fs"), P("tp"), weight, weight, P("tp", "fs"), P("tp"),
        ),
        out_specs=P("fs", None, "tp"),
        check_vma=False,
    )
```

```python
import functools

import jax
import jax.numpy as jnp
from jax import lax
from jax.experimental import pallas as pl
from jax.experimental.pallas import tpu as pltpu
from jax.sharding import PartitionSpec as P

ALPHA = 2.0**0.25
EPSILON = 1e-05
MESH = pl.DeviceIdType.MESH
F32 = jnp.float32
BF16 = jnp.bfloat16

CORES = 2
FIRST = (0, 1, 2)
CONV = (3, 4, 5)
LAST = (6, 7, 8)
DOWN = (2, 5, 8)


def flip(value, k, size):
    bit = 1
    while bit < size:
        if k & bit:
            value = value + bit - 2 * bit * ((value // bit) % 2)
        bit *= 2
    return value


def low(k):
    return k & -k


def bits_below(limit):
    bit = 1
    while bit < limit:
        yield bit
        bit *= 2


def layer_kernel(n_z, n_y, n_x, cuts, tokens_ref, *refs):
    weights = refs[:9]
    first_gain, conv_taps, conv_gain, second_gain, third_gain = refs[9:14]
    out_ref = refs[14]
    bufs = refs[15:24]
    xgs, hiddens = refs[24:26], refs[26:28]
    (xc, core_out, core_in, side_out, side_in, held, line_out, line_in,
     c_core_out, c_core_in, c_side_out, c_side_in, current, conv_in, acted, stat) = refs[28:44]
    (wz_s, wz_r, wy_s, wy_r, own_s, gz_s, gz_r, gx_s, gx_r, gc_s, gc_r,
     rc_s, rc_r, rx_s, rx_r, rz_s, rz_r, st_s, st_r) = refs[44:]

    n_tp = n_x * CORES
    fs = lax.axis_index("fs")
    tp = lax.axis_index("tp")
    z, y = fs // n_y, fs % n_y
    x, core = tp // CORES, tp % CORES
    length, width = tokens_ref.shape
    features = width * n_tp
    partner = (fs, x * CORES + 1 - core)

    def along(k):
        return (flip(z, k, n_z) * n_y + y, tp)


    barrier = pltpu.get_barrier_semaphore()
    for k in range(1, n_z):
        pl.semaphore_signal(barrier, inc=1, device_id=(flip(z, k, n_z) * n_y + y, tp), device_id_type=MESH)
    for o in range(1, n_y):
        pl.semaphore_signal(barrier, inc=1, device_id=(z * n_y + (y + o) % n_y, tp), device_id_type=MESH)
    for o in range(1, n_tp):
        pl.semaphore_signal(barrier, inc=1, device_id=(fs, (tp + o) % n_tp), device_id_type=MESH)
    pl.semaphore_wait(barrier, n_z - 1 + n_y - 1 + n_tp - 1)

    pending = {}

    def remote(src, dst, s, r, dest):
        return pltpu.make_async_remote_copy(
            src_ref=src, dst_ref=dst, send_sem=s, recv_sem=r, device_id=dest, device_id_type=MESH
        )

    def send(group, src, dst, s, r, dest):
        copy = remote(src, dst, s, r, dest)
        copy.start()
        pending.setdefault(group, []).append(copy)

    def arrive(dst, s, r):
        remote(dst, dst, s, r, (fs, tp)).wait_recv()

    def flush(*groups):
        for group in groups:
            for copy in pending.pop(group, []):
                copy.wait_send()

    def slot(m, block):
        if m in DOWN:
            return bufs[m].at[block]
        rows = bufs[m].shape[0] // (n_z * n_y)
        return bufs[m].at[pl.ds(pl.multiple_of(block * rows, 16), rows)]

    def part_of(m, zz):
        if m in CONV:
            return weights[m]
        place = zz % cuts[m in LAST]
        chunk = hiddens[m in LAST].shape[2]
        if m in DOWN:
            return weights[m].at[pl.ds(pl.multiple_of(place * chunk, 16), chunk)]
        if len(weights[m].shape) == 3:
            return weights[m].at[place]
        return weights[m].at[:, pl.ds(pl.multiple_of(place * chunk, 128), chunk)]

    def to_y(m, k, src):
        for o in range(1, n_y):
            send(
                "weights", src, slot(m, along(k)[0]), wy_s.at[m, k, o - 1], wy_r.at[m, k, o - 1],
                (z * n_y + (y + o) % n_y, tp),
            )

    def tree_send(group, k, src, dst, s, r):
        for bit in bits_below(low(k) if k else n_z):
            send(group, src, dst, s(k ^ bit), r(k ^ bit), along(bit))

    def weight_own(*matrices):
        for m in matrices:
            own = part_of(m, z)
            to_y(m, 0, own)
            pltpu.make_async_copy(own, slot(m, fs), own_s.at[m]).start()

    def unit_send(m, k):
        zz = flip(z, k, n_z)
        send("weights", part_of(m, zz), slot(m, fs), wz_s.at[m, k], wz_r.at[m, k], along(k))

    def unit_forward(m, k):
        block = slot(m, along(k)[0])
        arrive(block, wz_s.at[m, k], wz_r.at[m, k])
        to_y(m, k, block)

    def conv_start():
        for m in CONV:
            tree_send("weights", 0, weights[m], slot(m, fs), lambda k: wz_s.at[m, k], lambda k: wz_r.at[m, k])
        weight_own(*CONV)

    def conv_block(k):
        for m in CONV:
            block = slot(m, along(k)[0])
            arrive(block, wz_s.at[m, k], wz_r.at[m, k])
            tree_send("weights", k, block, block, lambda i: wz_s.at[m, i], lambda i: wz_r.at[m, i])
            to_y(m, k, block)

    def weight_ready(m):
        for k in range(n_z):
            zz = flip(z, k, n_z)
            for o in range(1, n_y):
                arrive(slot(m, zz * n_y + (y + n_y - o) % n_y), wy_s.at[m, k, o - 1], wy_r.at[m, k, o - 1])
        pltpu.make_async_copy(part_of(m, z), slot(m, fs), own_s.at[m]).wait()

    units = [(m, k) for m in FIRST for k in range(n_z - 1, 0, -1)]
    units += [(m, k) for m in LAST for k in (1, *range(n_z - 1, 1, -1))]
    sent, landed = [0], [0]

    def issue(count):
        for unit in units[sent[0] : sent[0] + count]:
            unit_send(*unit)
        sent[0] = min(sent[0] + count, len(units))

    def forward(count):
        for unit in units[landed[0] : landed[0] + count]:
            unit_forward(*unit)
        landed[0] = min(landed[0] + count, len(units))

    def until(*matrices):
        need = 1 + max((n for n, unit in enumerate(units) if unit[0] in matrices), default=-1)
        issue(max(need - sent[0], 0))
        forward(max(need - landed[0], 0))
        for m in matrices:
            weight_ready(m)

    def act(step):
        for fn, *args in step:
            fn(*args)

    def columns(t):
        return pl.ds(pl.multiple_of(t * width, 128), width)

    def spread(group, src, dst, x_s, x_r, c_s, c_r):
        for o in range(1, n_x):
            send(group, src, dst(tp), x_s(o - 1), x_r(o - 1), (fs, (x + o) % n_x * CORES + core))
        send(group, src, dst(tp), c_s(x), c_r(x), partner)

    def pass_on(group, dst, x_s, x_r, c_s, c_r):
        for o in range(1, n_x):
            xx = (x + n_x - o) % n_x
            block = dst(xx * CORES + core)
            arrive(block, x_s(o - 1), x_r(o - 1))
            send(group, block, block, c_s(xx), c_r(xx), partner)

    def collect(dst, x_s, x_r, c_s, c_r):
        for o in range(n_x):
            xx = (x + o) % n_x
            arrive(dst(xx * CORES + 1 - core), c_s(xx), c_r(xx))

    def seq_refs(f, k):
        return (
            lambda t: xgs[f].at[k, :, columns(t)],
            lambda i: gx_s.at[f, k, i], lambda i: gx_r.at[f, k, i],
            lambda i: gc_s.at[f, k, i], lambda i: gc_r.at[f, k, i],
        )

    def gather_start(f, src):
        group = ("gather", f)
        for bit in bits_below(cuts[f]):
            send(group, src, xgs[f].at[bit, :, columns(tp)], gz_s.at[f, bit], gz_r.at[f, bit], along(bit))
        spread(group, src, *seq_refs(f, 0))
        xgs[f][0, :, columns(tp)] = src[...]

    def gather_block(f, k):
        group = ("gather", f)
        block = xgs[f].at[k, :, columns(tp)]
        arrive(block, gz_s.at[f, k], gz_r.at[f, k])
        for bit in bits_below(low(k)):
            send(group, block, xgs[f].at[k ^ bit, :, columns(tp)], gz_s.at[f, k ^ bit], gz_r.at[f, k ^ bit], along(bit))
        spread(group, block, *seq_refs(f, k))

    def gather_pass(f, k):
        pass_on(("gather", f), *seq_refs(f, k))

    def ffn_hidden(f, k, gate, up):
        rows = xgs[f][k]
        g = jnp.dot(rows, gate[...], preferred_element_type=F32)
        u = jnp.dot(rows, up[...], preferred_element_type=F32)
        hiddens[f][k] = (g * jax.nn.sigmoid(g) * u).astype(BF16)

    def project(source, down, t):
        part = down.shape[2]
        per = width // part
        for q in range(per):
            yield slice(q * part, (q + 1) * part), jnp.dot(source[...], down[t * per + q], preferred_element_type=F32)

    def reduce_give(group, source, down, outgoing, incoming, s, r):
        for o in [*range(1, n_x), 0]:
            xx = (x + o) % n_x
            for cols, value in project(source, down, xx * CORES + 1 - core):
                outgoing(xx)[:, cols] = value.astype(BF16)
            send(group, outgoing(xx), incoming(xx), s(xx), r(xx), partner)

    def reduce_take(group, source, down, incoming, s, r, outgoing, target, xs, xr, keep):
        for o in [*range(1, n_x), 0]:
            xx = (x + o) % n_x
            arrive(incoming(xx), s(xx), r(xx))
            for cols, value in project(source, down, xx * CORES + core):
                total = value + incoming(xx)[:, cols].astype(F32)
                if o:
                    outgoing(o - 1)[:, cols] = total.astype(BF16)
                else:
                    keep[:, cols] = total
            if o:
                send(group, outgoing(o - 1), target(o - 1), xs(o - 1), xr(o - 1), (fs, xx * CORES + core))

    def reduce_sum(target, xs, xr, keep):
        total = keep[...]
        for o in range(1, n_x):
            arrive(target(o - 1), xs(o - 1), xr(o - 1))
            total = total + target(o - 1)[...].astype(F32)
        keep[...] = total

    def reduce_ffn(f, down, plan):
        group = ("reduce", f)

        def give(k):
            reduce_give(
                group, hiddens[f].at[k], down, lambda i: core_out.at[k, i], lambda i: core_in.at[k, i],
                lambda i: rc_s.at[f, k, i], lambda i: rc_r.at[f, k, i],
            )

        def take(k):
            reduce_take(
                group, hiddens[f].at[k], down, lambda i: core_in.at[k, i],
                lambda i: rc_s.at[f, k, i], lambda i: rc_r.at[f, k, i],
                lambda i: side_out.at[k, i], lambda i: side_in.at[k, i],
                lambda i: rx_s.at[f, k, i], lambda i: rx_r.at[f, k, i], held.at[k],
            )

        give(cuts[f] - 1)
        for k in range(cuts[f] - 1, -1, -1):
            if k:
                give(k - 1)
            take(k)
        act(plan.get("given", ()))
        for k in range(cuts[f] - 1, -1, -1):
            act(plan.get(k, ()))
            reduce_sum(
                lambda i: side_in.at[k, i], lambda i: rx_s.at[f, k, i], lambda i: rx_r.at[f, k, i], held.at[k]
            )
            total = held[k]
            for bit in bits_below(low(k) if k else cuts[f]):
                i = (k ^ bit) - 1
                arrive(line_in.at[i], rz_s.at[f, i], rz_r.at[f, i])
                total = total + line_in[i].astype(F32)
            if k == 0:
                return total
            line_out[k - 1] = total.astype(BF16)
            send(group, line_out.at[k - 1], line_in.at[k - 1], rz_s.at[f, k - 1], rz_r.at[f, k - 1], along(low(k)))

    def stats_start(phase, values):
        sums = jnp.sum(values, axis=-1, keepdims=True)
        squares = jnp.sum(values * values, axis=-1, keepdims=True)
        lane = lax.broadcasted_iota(jnp.int32, (values.shape[0], 128), 1)
        both = jnp.where(lane == 0, sums, jnp.where(lane == 1, squares, 0.0))
        stat[phase, n_tp - 1] = both.T[:8]
        for step in range(1, n_tp):
            i = step - 1
            remote(
                stat.at[phase, n_tp - 1], stat.at[phase, i], st_s.at[phase, i], st_r.at[phase, i],
                (fs, (tp + step) % n_tp),
            ).start()

    def stats_wait(phase, all_width):
        for step in range(1, n_tp):
            i = step - 1
            remote(
                stat.at[phase, n_tp - 1], stat.at[phase, i], st_s.at[phase, i], st_r.at[phase, i], (fs, tp)
            ).wait()
        total = stat[phase, 0]
        for i in range(1, n_tp):
            total = total + stat[phase, i]
        both = jnp.concatenate([total] * 16, axis=0).T
        center = both[:, 0:1] / all_width
        spread_of = both[:, 1:2] / all_width - center * center
        return center, lax.rsqrt(spread_of + EPSILON)

    def row_of(gain):
        return gain[...].astype(F32).reshape(1, gain.shape[0])

    def post_norm(phase, gain):
        stats_start(phase, current[...])
        center, scale = stats_wait(phase, features)
        return ((current[...] - center) * scale * row_of(gain)).astype(BF16)

    gather_start(0, tokens_ref)
    weight_own(*FIRST, *LAST[:2])
    issue(3)
    gather_block(0, 1)
    issue(1)
    gather_block(0, 2)
    issue(2)
    gather_pass(0, 0)
    forward(2)
    gather_block(0, 3)
    issue(3)
    conv_start()
    issue(2)
    gather_pass(0, 1)
    forward(1)
    gather_pass(0, 2)
    forward(1)
    gather_pass(0, 3)
    for k in range(n_z):
        collect(*seq_refs(0, k))
    until(0, 1)
    forward(2)
    for low_k, high_k in ((0, n_z // 2), (n_z // 2, n_z)):
        lax.fori_loop(low_k, high_k, lambda i, c: (ffn_hidden(0, i, bufs[0], bufs[1]), c)[1], 0)
        forward(1 if low_k == 0 else 0)
    until(2)
    current[...] = ALPHA * tokens_ref[...].astype(F32) + 0.5 * reduce_ffn(0, bufs[2], {
        "given": [(conv_block, 1), (conv_block, 2), (issue, 1)],
        2: [(forward, 1)],
        1: [(forward, 1), (weight_own, LAST[2])],
    })
    issue(2)
    forward(1)
    first = post_norm(0, first_gain)
    out_ref[...] = first

    conv_refs = (
        lambda t: xc.at[:, columns(t)],
        lambda i: gx_s.at[2, 0, i], lambda i: gx_r.at[2, 0, i],
        lambda i: gc_s.at[2, 0, i], lambda i: gc_r.at[2, 0, i],
    )
    spread("conv", out_ref, *conv_refs)
    xc[:, columns(tp)] = first
    conv_block(3)
    forward(1)
    issue(1)
    pass_on("conv", *conv_refs)
    until(3, 4)
    collect(*conv_refs)

    channels = acted.shape[1]
    taps = conv_taps.shape[0]
    reach = (taps - 1) // 2
    margin = (conv_in.shape[0] - length) // 2
    rows = xc[...]
    value = jnp.dot(rows, bufs[3][...], preferred_element_type=F32)
    gate = jnp.dot(rows, bufs[4][...], preferred_element_type=F32)
    conv_in[0:margin] = jnp.zeros((margin, channels), F32)
    conv_in[margin + length :] = jnp.zeros((margin, channels), F32)
    conv_in[margin : margin + length] = value * jax.nn.sigmoid(gate)
    rows_each = length // 4
    for top in range(0, length, rows_each):
        for left in range(0, channels, 128):
            cols = slice(left, left + 128)
            total = jnp.zeros((rows_each, 128), F32)
            for tap in range(taps):
                start = margin - reach + top + tap
                total = total + conv_taps[tap : tap + 1, cols].astype(F32) * conv_in[start : start + rows_each, cols]
            current[top : top + rows_each, cols] = total
    stats_start(1, current[:, 0:channels])
    center, scale = stats_wait(1, channels * n_tp)
    normed = (current[:, 0:channels] - center) * scale * row_of(conv_gain)
    acted[...] = (normed * jax.nn.sigmoid(normed)).astype(BF16)
    until(5)
    conv_core = (lambda i: rc_s.at[2, 0, i], lambda i: rc_r.at[2, 0, i])
    conv_side = (lambda i: rx_s.at[2, 0, i], lambda i: rx_r.at[2, 0, i])
    reduce_give("conv", acted, bufs[5], lambda i: c_core_out.at[i], lambda i: c_core_in.at[i], *conv_core)
    issue(2)
    reduce_take(
        "conv", acted, bufs[5], lambda i: c_core_in.at[i], *conv_core,
        lambda i: c_side_out.at[i], lambda i: c_side_in.at[i], *conv_side, current,
    )
    forward(1)
    reduce_sum(lambda i: c_side_in.at[i], *conv_side, current)
    current[...] = ALPHA * out_ref[...].astype(F32) + current[...]
    second = post_norm(2, second_gain)
    flush("conv")
    out_ref[...] = second

    gather_start(1, out_ref)
    issue(1)
    forward(2)
    gather_block(1, 1)
    forward(1)
    gather_pass(1, 0)
    until(6, 7)
    collect(*seq_refs(1, 0))
    ffn_hidden(1, 0, bufs[6], bufs[7])
    forward(1)
    for k in range(1, cuts[1]):
        if k > 1:
            gather_block(1, k)
        gather_pass(1, k)
        collect(*seq_refs(1, k))
        ffn_hidden(1, k, bufs[6], bufs[7])
    until(8)
    flush(("reduce", 0))
    current[...] = ALPHA * out_ref[...].astype(F32) + 0.5 * reduce_ffn(1, bufs[8], {})
    normed = post_norm(3, third_gain)
    flush("weights", ("gather", 0), ("gather", 1), ("reduce", 1))
    out_ref[...] = normed


def solution(mesh):
    n_fs, n_tp = mesh.shape["fs"], mesh.shape["tp"]
    n_y = 1 << ((n_fs.bit_length() - 1) // 2)
    n_z, n_x = n_fs // n_y, n_tp // CORES

    def body(
        tokens, first_gate, first_up, first_down, first_gain, glu_value, glu_gate, conv_taps, conv_gain,
        conv_proj, second_gain, last_gate, last_up, last_down, third_gain,
    ):
        tokens = tokens[0]
        length, width = tokens.shape
        features = width * n_tp
        cuts = (n_z, min(n_z, 2))
        chunks = [first_gate.shape[1] // cut for cut in cuts]

        def by_chunk(w, f):
            if chunks[f] % 128 == 0:
                return w
            return jnp.swapaxes(w.reshape(w.shape[0], cuts[f], chunks[f]), 0, 1)

        weights = (
            by_chunk(first_gate, 0), by_chunk(first_up, 0), first_down, glu_value, glu_gate, conv_proj,
            by_chunk(last_gate, 1), by_chunk(last_up, 1), last_down,
        )
        channels = glu_value.shape[1]
        reach = (conv_taps.shape[0] - 1) // 2
        margin = -(-reach // 8) * 8
        part = first_down.shape[1]
        wide = [pltpu.VMEM((features, chunk), BF16) for chunk in chunks]
        down = [pltpu.VMEM((n_fs, chunk, part), BF16) for chunk in chunks]
        glu = pltpu.VMEM((features, channels), BF16)
        proj = pltpu.VMEM((n_fs, channels, part), BF16)
        dma = pltpu.SemaphoreType.DMA
        vmem = pl.BlockSpec(memory_space=pltpu.VMEM)
        others, others_z = max(n_x - 1, 1), max(n_z - 1, 1)

        def blocks(*lead, kind=BF16):
            return pltpu.VMEM(lead + (length, width), kind)

        def pair(*shape):
            return [dma(shape), dma(shape)]

        result = pl.pallas_call(
            functools.partial(layer_kernel, n_z, n_y, n_x, cuts),
            out_shape=jax.ShapeDtypeStruct((length, width), BF16),
            in_specs=[vmem] + [pl.BlockSpec(memory_space=pl.ANY)] * 9 + [vmem] * 5,
            out_specs=vmem,
            scratch_shapes=[wide[0], wide[0], down[0], glu, glu, proj, wide[1], wide[1], down[1]]
            + [pltpu.VMEM((cut, length, features), BF16) for cut in cuts]
            + [pltpu.VMEM((cut, length, chunk), BF16) for cut, chunk in zip(cuts, chunks)]
            + [
                pltpu.VMEM((length, features), BF16),
                blocks(n_z, n_x),
                blocks(n_z, n_x),
                blocks(n_z, others),
                blocks(n_z, others),
                blocks(n_z, kind=F32),
                blocks(others_z),
                blocks(others_z),
                blocks(n_x),
                blocks(n_x),
                blocks(others),
                blocks(others),
                blocks(kind=F32),
                pltpu.VMEM((length + 2 * margin, channels), F32),
                pltpu.VMEM((length, channels), BF16),
                pltpu.VMEM((4, n_tp, 8, length), F32),
            ]
            + pair(9, n_z)
            + pair(9, n_z, max(n_y - 1, 1))
            + [dma((9,))]
            + pair(2, n_z)
            + pair(3, n_z, others)
            + pair(3, n_z, n_x)
            + pair(3, n_z, n_x)
            + pair(3, n_z, others)
            + pair(2, others_z)
            + pair(4, n_tp - 1),
            compiler_params=pltpu.CompilerParams(
                collective_id=0, has_side_effects=True, vmem_limit_bytes=67000000
            ),
        )(
            tokens, *weights, first_gain, conv_taps, conv_gain, second_gain, third_gain
        )
        return result[None]

    weight = P("fs", "tp")
    return jax.shard_map(
        body,
        mesh=mesh,
        in_specs=(
            P("fs", None, "tp"), weight, weight, P("tp", "fs"), P("tp"), weight, weight, P(None, "tp"), P("tp"),
            P("tp", "fs"), P("tp"), weight, weight, P("tp", "fs"), P("tp"),
        ),
        out_specs=P("fs", None, "tp"),
        check_vma=False,
    )
```

```python
import functools

import jax
import jax.numpy as jnp
from jax import lax
from jax.experimental import pallas as pl
from jax.experimental.pallas import tpu as pltpu
from jax.sharding import PartitionSpec as P

ALPHA = 2.0**0.25
EPSILON = 1e-05
MESH = pl.DeviceIdType.MESH
F32 = jnp.float32
BF16 = jnp.bfloat16

CORES = 2
FIRST = (0, 1, 2)
CONV = (3, 4, 5)
LAST = (6, 7, 8)
DOWN = (2, 5, 8)


def flip(value, k, size):
    bit = 1
    while bit < size:
        if k & bit:
            value = value + bit - 2 * bit * ((value // bit) % 2)
        bit *= 2
    return value


def low(k):
    return k & -k


def bits_below(limit):
    bit = 1
    while bit < limit:
        yield bit
        bit *= 2


def layer_kernel(n_z, n_y, n_x, cuts, tokens_ref, *refs):
    weights = refs[:9]
    first_gain, conv_taps, conv_gain, second_gain, third_gain = refs[9:14]
    out_ref = refs[14]
    bufs = refs[15:24]
    xgs, hiddens = refs[24:26], refs[26:28]
    (xc, core_out, core_in, side_out, side_in, held, line_out, line_in,
     c_core_out, c_core_in, c_side_out, c_side_in, current, conv_in, acted, stat) = refs[28:44]
    (wz_s, wz_r, wy_s, wy_r, own_s, gz_s, gz_r, gx_s, gx_r, gc_s, gc_r,
     rc_s, rc_r, rx_s, rx_r, rz_s, rz_r, st_s, st_r) = refs[44:]

    n_tp = n_x * CORES
    fs = lax.axis_index("fs")
    tp = lax.axis_index("tp")
    z, y = fs // n_y, fs % n_y
    x, core = tp // CORES, tp % CORES
    length, width = tokens_ref.shape
    features = width * n_tp
    partner = (fs, x * CORES + 1 - core)

    def along(k):
        return (flip(z, k, n_z) * n_y + y, tp)


    barrier = pltpu.get_barrier_semaphore()
    for k in range(1, n_z):
        pl.semaphore_signal(barrier, inc=1, device_id=(flip(z, k, n_z) * n_y + y, tp), device_id_type=MESH)
    for o in range(1, n_y):
        pl.semaphore_signal(barrier, inc=1, device_id=(z * n_y + (y + o) % n_y, tp), device_id_type=MESH)
    for o in range(1, n_tp):
        pl.semaphore_signal(barrier, inc=1, device_id=(fs, (tp + o) % n_tp), device_id_type=MESH)
    pl.semaphore_wait(barrier, n_z - 1 + n_y - 1 + n_tp - 1)

    pending = {}

    def remote(src, dst, s, r, dest):
        return pltpu.make_async_remote_copy(
            src_ref=src, dst_ref=dst, send_sem=s, recv_sem=r, device_id=dest, device_id_type=MESH
        )

    def send(group, src, dst, s, r, dest):
        copy = remote(src, dst, s, r, dest)
        copy.start()
        pending.setdefault(group, []).append(copy)

    def arrive(dst, s, r):
        remote(dst, dst, s, r, (fs, tp)).wait_recv()

    def flush(*groups):
        for group in groups:
            for copy in pending.pop(group, []):
                copy.wait_send()

    def slot(m, block):
        if m in DOWN:
            return bufs[m].at[block]
        rows = bufs[m].shape[0] // (n_z * n_y)
        return bufs[m].at[pl.ds(pl.multiple_of(block * rows, 16), rows)]

    def part_of(m, zz):
        if m in CONV:
            return weights[m]
        place = zz % cuts[m in LAST]
        chunk = hiddens[m in LAST].shape[2]
        if m in DOWN:
            return weights[m].at[pl.ds(pl.multiple_of(place * chunk, 16), chunk)]
        if len(weights[m].shape) == 3:
            return weights[m].at[place]
        return weights[m].at[:, pl.ds(pl.multiple_of(place * chunk, 128), chunk)]

    units = [(m, k, 0) for m in FIRST for k in range(n_z - 1, 0, -1)]
    units += [(m, k, 0) for m in LAST for k in (1, *range(n_z - 1, 1, -1))]
    halved = units[-1][:2]
    units.append((*halved, 1))

    def half(ref, m, k, j):
        if (m, k) != halved:
            return ref
        rows = ref.shape[0] // 2
        return ref.at[pl.ds(j * rows, rows)]

    def z_sems(m, k, j=0):
        i = 9 * (n_z - 1) if j else m * (n_z - 1) + k - 1
        return wz_s.at[i], wz_r.at[i]

    def y_sems(m, k, j, o):
        i = 9 * n_z if j else m * n_z + k
        return wy_s.at[i, o - 1], wy_r.at[i, o - 1]

    def to_y(m, k, src, j=0):
        for o in range(1, n_y):
            dst = half(slot(m, along(k)[0]), m, k, j)
            send("weights", src, dst, *y_sems(m, k, j, o), (z * n_y + (y + o) % n_y, tp))

    def tree_send(group, k, src, dst, s, r):
        for bit in bits_below(low(k) if k else n_z):
            send(group, src, dst, s(k ^ bit), r(k ^ bit), along(bit))

    def weight_own(*matrices):
        for m in matrices:
            own = part_of(m, z)
            to_y(m, 0, own)
            pltpu.make_async_copy(own, slot(m, fs), own_s.at[m]).start()

    def unit_send(m, k, j):
        src = half(part_of(m, flip(z, k, n_z)), m, k, j)
        send("weights", src, half(slot(m, fs), m, k, j), *z_sems(m, k, j), along(k))

    def unit_forward(m, k, j):
        block = half(slot(m, along(k)[0]), m, k, j)
        arrive(block, *z_sems(m, k, j))
        to_y(m, k, block, j)

    def conv_start():
        for m in CONV:
            tree_send("weights", 0, weights[m], slot(m, fs), lambda k: z_sems(m, k)[0], lambda k: z_sems(m, k)[1])
        weight_own(*CONV)

    def conv_block(k):
        for m in CONV:
            block = slot(m, along(k)[0])
            arrive(block, *z_sems(m, k))
            tree_send("weights", k, block, block, lambda i: z_sems(m, i)[0], lambda i: z_sems(m, i)[1])
            to_y(m, k, block)

    def weight_ready(m):
        for k in range(n_z):
            zz = flip(z, k, n_z)
            for o in range(1, n_y):
                block = slot(m, zz * n_y + (y + n_y - o) % n_y)
                for j in range(1 + ((m, k) == halved)):
                    arrive(half(block, m, k, j), *y_sems(m, k, j, o))
        pltpu.make_async_copy(part_of(m, z), slot(m, fs), own_s.at[m]).wait()

    sent, landed = [0], [0]

    def issue(count):
        for unit in units[sent[0] : sent[0] + count]:
            unit_send(*unit)
        sent[0] = min(sent[0] + count, len(units))

    def forward(count):
        for unit in units[landed[0] : landed[0] + count]:
            unit_forward(*unit)
        landed[0] = min(landed[0] + count, len(units))

    def until(*matrices):
        need = 1 + max((n for n, unit in enumerate(units) if unit[0] in matrices), default=-1)
        issue(max(need - sent[0], 0))
        forward(max(need - landed[0], 0))
        for m in matrices:
            weight_ready(m)

    def act(step):
        for fn, *args in step:
            fn(*args)

    def columns(t):
        return pl.ds(pl.multiple_of(t * width, 128), width)

    def spread(group, src, dst, x_s, x_r, c_s, c_r):
        for o in range(1, n_x):
            send(group, src, dst(tp), x_s(o - 1), x_r(o - 1), (fs, (x + o) % n_x * CORES + core))
        send(group, src, dst(tp), c_s(x), c_r(x), partner)

    def pass_on(group, dst, x_s, x_r, c_s, c_r):
        for o in range(1, n_x):
            xx = (x + n_x - o) % n_x
            block = dst(xx * CORES + core)
            arrive(block, x_s(o - 1), x_r(o - 1))
            send(group, block, block, c_s(xx), c_r(xx), partner)

    def collect(dst, x_s, x_r, c_s, c_r):
        for o in range(n_x):
            xx = (x + o) % n_x
            arrive(dst(xx * CORES + 1 - core), c_s(xx), c_r(xx))

    def seq_refs(f, k):
        b = f * n_z + k
        return (
            lambda t: xgs[f].at[k, :, columns(t)],
            lambda i: gx_s.at[b, i], lambda i: gx_r.at[b, i],
            lambda i: gc_s.at[b, i], lambda i: gc_r.at[b, i],
        )

    def line_sems(f, k):
        return gz_s.at[f * (n_z - 1) + k - 1], gz_r.at[f * (n_z - 1) + k - 1]

    def gather_start(f, src):
        group = ("gather", f)
        for bit in bits_below(cuts[f]):
            send(group, src, xgs[f].at[bit, :, columns(tp)], *line_sems(f, bit), along(bit))
        spread(group, src, *seq_refs(f, 0))
        xgs[f][0, :, columns(tp)] = src[...]

    def gather_block(f, k):
        group = ("gather", f)
        block = xgs[f].at[k, :, columns(tp)]
        arrive(block, *line_sems(f, k))
        for bit in bits_below(low(k)):
            send(group, block, xgs[f].at[k ^ bit, :, columns(tp)], *line_sems(f, k ^ bit), along(bit))
        spread(group, block, *seq_refs(f, k))

    def gather_pass(f, k):
        pass_on(("gather", f), *seq_refs(f, k))

    def ffn_hidden(f, k, gate, up):
        rows = xgs[f][k]
        g = jnp.dot(rows, gate[...], preferred_element_type=F32)
        u = jnp.dot(rows, up[...], preferred_element_type=F32)
        hiddens[f][k] = (g * jax.nn.sigmoid(g) * u).astype(BF16)

    def project(source, down, t):
        part = down.shape[2]
        per = width // part
        for q in range(per):
            yield slice(q * part, (q + 1) * part), jnp.dot(source[...], down[t * per + q], preferred_element_type=F32)

    def reduce_give(group, source, down, outgoing, incoming, s, r):
        for o in [*range(1, n_x), 0]:
            xx = (x + o) % n_x
            for cols, value in project(source, down, xx * CORES + 1 - core):
                outgoing(xx)[:, cols] = value.astype(BF16)
            send(group, outgoing(xx), incoming(xx), s(xx), r(xx), partner)

    def reduce_take(group, source, down, incoming, s, r, outgoing, target, xs, xr, keep):
        for o in [*range(1, n_x), 0]:
            xx = (x + o) % n_x
            arrive(incoming(xx), s(xx), r(xx))
            for cols, value in project(source, down, xx * CORES + core):
                total = value + incoming(xx)[:, cols].astype(F32)
                if o:
                    outgoing(o - 1)[:, cols] = total.astype(BF16)
                else:
                    keep[:, cols] = total
            if o:
                send(group, outgoing(o - 1), target(o - 1), xs(o - 1), xr(o - 1), (fs, xx * CORES + core))

    def reduce_sum(target, xs, xr, keep):
        total = keep[...]
        for o in range(1, n_x):
            arrive(target(o - 1), xs(o - 1), xr(o - 1))
            total = total + target(o - 1)[...].astype(F32)
        keep[...] = total

    def reduce_ffn(f, down, plan):
        group = ("reduce", f)

        def give(k):
            reduce_give(
                group, hiddens[f].at[k], down, lambda i: core_out.at[k, i], lambda i: core_in.at[k, i],
                lambda i: rc_s.at[f * n_z + k, i], lambda i: rc_r.at[f * n_z + k, i],
            )

        def take(k):
            reduce_take(
                group, hiddens[f].at[k], down, lambda i: core_in.at[k, i],
                lambda i: rc_s.at[f * n_z + k, i], lambda i: rc_r.at[f * n_z + k, i],
                lambda i: side_out.at[k, i], lambda i: side_in.at[k, i],
                lambda i: rx_s.at[f * n_z + k, i], lambda i: rx_r.at[f * n_z + k, i], held.at[k],
            )

        def line_add(k, i):
            arrive(line_in.at[i], rz_s.at[f * (n_z - 1)], rz_r.at[f * n_z + i])
            held[k] = held[k] + line_in[i].astype(F32)

        def line_copy(k, i, dest):
            return remote(line_out.at[k - 1], line_in.at[i], rz_s.at[f * (n_z - 1) + k - 1], rz_r.at[f * n_z + i], along(dest))

        def line_go(k, i, dest):
            line_out[k - 1] = held[k].astype(BF16)
            line_copy(k, i, dest).start()

        def line_tree(k):
            for bit in bits_below(low(k) if k else cuts[f]):
                line_add(k, (k ^ bit) - 1)
            if k:
                line_go(k, k - 1, low(k))
                pending.setdefault(group, []).append(line_copy(k, k - 1, low(k)))

        def line_inner(k):
            inner = (z + 1) // 2 % 2

            def outer_far():
                line_go(k, 5 - k, 1)

            def inner_near():
                line_add(2, 2)
                line_go(2, 1, 2)

            def inner_far():
                line_add(3, 3)
                line_go(3, 1, 3)

            if k > 1:
                pl.when(inner == 0)(outer_far)
            if k == 2:
                pl.when(inner == 1)(inner_near)
            if k == 1:
                line_go(1, 0, 1)
                pl.when(inner == 1)(inner_far)
            if k == 0:
                line_add(0, 0)
                line_add(0, 1)
            else:
                pending.setdefault(group, []).append(line_copy(k, 0, 1))

        give(cuts[f] - 1)
        for k in range(cuts[f] - 1, -1, -1):
            if k:
                give(k - 1)
            take(k)
        act(plan.get("given", ()))
        for k in range(cuts[f] - 1, -1, -1):
            act(plan.get(k, ()))
            reduce_sum(
                lambda i: side_in.at[k, i], lambda i: rx_s.at[f * n_z + k, i], lambda i: rx_r.at[f * n_z + k, i], held.at[k]
            )
            if cuts[f] == 4:
                line_inner(k)
            else:
                line_tree(k)
        return held[0]

    def stats_start(phase, values):
        sums = jnp.sum(values, axis=-1, keepdims=True)
        squares = jnp.sum(values * values, axis=-1, keepdims=True)
        lane = lax.broadcasted_iota(jnp.int32, (values.shape[0], 128), 1)
        both = jnp.where(lane == 0, sums, jnp.where(lane == 1, squares, 0.0))
        stat[phase, n_tp - 1] = both.T[:8]
        for step in range(1, n_tp):
            i = step - 1
            remote(
                stat.at[phase, n_tp - 1], stat.at[phase, i], st_s.at[phase, i], st_r.at[phase, i],
                (fs, (tp + step) % n_tp),
            ).start()

    def stats_wait(phase, all_width):
        for step in range(1, n_tp):
            i = step - 1
            remote(
                stat.at[phase, n_tp - 1], stat.at[phase, i], st_s.at[phase, i], st_r.at[phase, i], (fs, tp)
            ).wait()
        total = stat[phase, 0]
        for i in range(1, n_tp):
            total = total + stat[phase, i]
        both = jnp.concatenate([total] * 16, axis=0).T
        center = both[:, 0:1] / all_width
        spread_of = both[:, 1:2] / all_width - center * center
        return center, lax.rsqrt(spread_of + EPSILON)

    def row_of(gain):
        return gain[...].astype(F32).reshape(1, gain.shape[0])

    def post_norm(phase, gain):
        stats_start(phase, current[...])
        center, scale = stats_wait(phase, features)
        return ((current[...] - center) * scale * row_of(gain)).astype(BF16)

    gather_start(0, tokens_ref)
    weight_own(*FIRST, *LAST[:2])
    issue(3)
    gather_block(0, 1)
    issue(1)
    gather_block(0, 2)
    issue(2)
    gather_pass(0, 0)
    forward(2)
    gather_block(0, 3)
    issue(3)
    conv_start()
    issue(2)
    gather_pass(0, 1)
    forward(1)
    gather_pass(0, 2)
    forward(1)
    gather_pass(0, 3)
    for k in range(n_z):
        collect(*seq_refs(0, k))
    until(0, 1)
    forward(2)
    for low_k, high_k in ((0, n_z // 2), (n_z // 2, n_z)):
        lax.fori_loop(low_k, high_k, lambda i, c: (ffn_hidden(0, i, bufs[0], bufs[1]), c)[1], 0)
        forward(1 if low_k == 0 else 0)
    until(2)
    current[...] = ALPHA * tokens_ref[...].astype(F32) + 0.5 * reduce_ffn(0, bufs[2], {
        "given": [(conv_block, 1), (conv_block, 2), (issue, 1)],
        2: [(forward, 1)],
        1: [(forward, 1), (weight_own, LAST[2])],
    })
    issue(2)
    forward(1)
    first = post_norm(0, first_gain)
    out_ref[...] = first

    conv_refs = (
        lambda t: xc.at[:, columns(t)],
        lambda i: gx_s.at[n_z + cuts[1], i], lambda i: gx_r.at[n_z + cuts[1], i],
        lambda i: gc_s.at[n_z + cuts[1], i], lambda i: gc_r.at[n_z + cuts[1], i],
    )
    spread("conv", out_ref, *conv_refs)
    xc[:, columns(tp)] = first
    conv_block(3)
    forward(1)
    issue(1)
    pass_on("conv", *conv_refs)
    until(3, 4)
    collect(*conv_refs)

    channels = acted.shape[1]
    taps = conv_taps.shape[0]
    reach = (taps - 1) // 2
    margin = (conv_in.shape[0] - length) // 2
    rows = xc[...]
    value = jnp.dot(rows, bufs[3][...], preferred_element_type=F32)
    gate = jnp.dot(rows, bufs[4][...], preferred_element_type=F32)
    conv_in[0:margin] = jnp.zeros((margin, channels), F32)
    conv_in[margin + length :] = jnp.zeros((margin, channels), F32)
    conv_in[margin : margin + length] = value * jax.nn.sigmoid(gate)
    rows_each = length // 4
    for top in range(0, length, rows_each):
        for left in range(0, channels, 128):
            cols = slice(left, left + 128)
            total = jnp.zeros((rows_each, 128), F32)
            for tap in range(taps):
                start = margin - reach + top + tap
                total = total + conv_taps[tap : tap + 1, cols].astype(F32) * conv_in[start : start + rows_each, cols]
            current[top : top + rows_each, cols] = total
    stats_start(1, current[:, 0:channels])
    center, scale = stats_wait(1, channels * n_tp)
    normed = (current[:, 0:channels] - center) * scale * row_of(conv_gain)
    acted[...] = (normed * jax.nn.sigmoid(normed)).astype(BF16)
    until(5)
    conv_core = (lambda i: rc_s.at[n_z + cuts[1], i], lambda i: rc_r.at[n_z + cuts[1], i])
    conv_side = (lambda i: rx_s.at[n_z + cuts[1], i], lambda i: rx_r.at[n_z + cuts[1], i])
    reduce_give("conv", acted, bufs[5], lambda i: c_core_out.at[i], lambda i: c_core_in.at[i], *conv_core)
    issue(2)
    reduce_take(
        "conv", acted, bufs[5], lambda i: c_core_in.at[i], *conv_core,
        lambda i: c_side_out.at[i], lambda i: c_side_in.at[i], *conv_side, current,
    )
    forward(1)
    reduce_sum(lambda i: c_side_in.at[i], *conv_side, current)
    current[...] = ALPHA * out_ref[...].astype(F32) + current[...]
    second = post_norm(2, second_gain)
    flush("conv")
    out_ref[...] = second

    gather_start(1, out_ref)
    issue(2)
    forward(2)
    gather_block(1, 1)
    forward(1)
    gather_pass(1, 0)
    until(6, 7)
    collect(*seq_refs(1, 0))
    ffn_hidden(1, 0, bufs[6], bufs[7])
    forward(2)
    for k in range(1, cuts[1]):
        if k > 1:
            gather_block(1, k)
        gather_pass(1, k)
        collect(*seq_refs(1, k))
        ffn_hidden(1, k, bufs[6], bufs[7])
    until(8)
    flush(("reduce", 0))
    current[...] = ALPHA * out_ref[...].astype(F32) + 0.5 * reduce_ffn(1, bufs[8], {})
    normed = post_norm(3, third_gain)
    flush("weights", ("gather", 0), ("gather", 1), ("reduce", 1))
    out_ref[...] = normed


def solution(mesh):
    n_fs, n_tp = mesh.shape["fs"], mesh.shape["tp"]
    n_y = 1 << ((n_fs.bit_length() - 1) // 2)
    n_z, n_x = n_fs // n_y, n_tp // CORES

    def body(
        tokens, first_gate, first_up, first_down, first_gain, glu_value, glu_gate, conv_taps, conv_gain,
        conv_proj, second_gain, last_gate, last_up, last_down, third_gain,
    ):
        tokens = tokens[0]
        length, width = tokens.shape
        features = width * n_tp
        cuts = (n_z, min(n_z, 2))
        chunks = [first_gate.shape[1] // cut for cut in cuts]

        def by_chunk(w, f):
            if chunks[f] % 128 == 0:
                return w
            return jnp.swapaxes(w.reshape(w.shape[0], cuts[f], chunks[f]), 0, 1)

        weights = (
            by_chunk(first_gate, 0), by_chunk(first_up, 0), first_down, glu_value, glu_gate, conv_proj,
            by_chunk(last_gate, 1), by_chunk(last_up, 1), last_down,
        )
        channels = glu_value.shape[1]
        reach = (conv_taps.shape[0] - 1) // 2
        margin = -(-reach // 8) * 8
        part = first_down.shape[1]
        wide = [pltpu.VMEM((features, chunk), BF16) for chunk in chunks]
        down = [pltpu.VMEM((n_fs, chunk, part), BF16) for chunk in chunks]
        glu = pltpu.VMEM((features, channels), BF16)
        proj = pltpu.VMEM((n_fs, channels, part), BF16)
        dma = pltpu.SemaphoreType.DMA
        vmem = pl.BlockSpec(memory_space=pltpu.VMEM)
        others = max(n_x - 1, 1)
        blocks_in_all = n_z + cuts[1] + 1

        def blocks(*lead, kind=BF16):
            return pltpu.VMEM(lead + (length, width), kind)

        def pair(*shape):
            return [dma(shape), dma(shape)]

        result = pl.pallas_call(
            functools.partial(layer_kernel, n_z, n_y, n_x, cuts),
            out_shape=jax.ShapeDtypeStruct((length, width), BF16),
            in_specs=[vmem] + [pl.BlockSpec(memory_space=pl.ANY)] * 9 + [vmem] * 5,
            out_specs=vmem,
            scratch_shapes=[wide[0], wide[0], down[0], glu, glu, proj, wide[1], wide[1], down[1]]
            + [pltpu.VMEM((cut, length, features), BF16) for cut in cuts]
            + [pltpu.VMEM((cut, length, chunk), BF16) for cut, chunk in zip(cuts, chunks)]
            + [
                pltpu.VMEM((length, features), BF16),
                blocks(n_z, n_x),
                blocks(n_z, n_x),
                blocks(n_z, others),
                blocks(n_z, others),
                blocks(n_z, kind=F32),
                blocks(n_z),
                blocks(n_z),
                blocks(n_x),
                blocks(n_x),
                blocks(others),
                blocks(others),
                blocks(kind=F32),
                pltpu.VMEM((length + 2 * margin, channels), F32),
                pltpu.VMEM((length, channels), BF16),
                pltpu.VMEM((4, n_tp, 8, length), F32),
            ]
            + pair(9 * (n_z - 1) + 1)
            + pair(9 * n_z + 1, max(n_y - 1, 1))
            + [dma((9,))]
            + pair(n_z + cuts[1] - 2)
            + pair(blocks_in_all, others)
            + pair(blocks_in_all, n_x)
            + pair(blocks_in_all, n_x)
            + pair(blocks_in_all, others)
            + [dma((n_z + cuts[1] - 2,)), dma((n_z + cuts[1] - 1,))]
            + pair(4, n_tp - 1),
            compiler_params=pltpu.CompilerParams(
                collective_id=0, has_side_effects=True, vmem_limit_bytes=67000000
            ),
        )(
            tokens, *weights, first_gain, conv_taps, conv_gain, second_gain, third_gain
        )
        return result[None]

    weight = P("fs", "tp")
    return jax.shard_map(
        body,
        mesh=mesh,
        in_specs=(
            P("fs", None, "tp"), weight, weight, P("tp", "fs"), P("tp"), weight, weight, P(None, "tp"), P("tp"),
            P("tp", "fs"), P("tp"), weight, weight, P("tp", "fs"), P("tp"),
        ),
        out_specs=P("fs", None, "tp"),
        check_vma=False,
    )
```

```python
import functools

import jax
import jax.numpy as jnp
from jax import lax
from jax.experimental import pallas as pl
from jax.experimental.pallas import tpu as pltpu
from jax.sharding import PartitionSpec as P

ALPHA = 2.0**0.25
EPSILON = 1e-05
MESH = pl.DeviceIdType.MESH
F32 = jnp.float32
BF16 = jnp.bfloat16

CORES = 2
FIRST = (0, 1, 2)
CONV = (3, 4, 5)
LAST = (6, 7, 8)
DOWN = (2, 5, 8)


def flip(value, k, size):
    bit = 1
    while bit < size:
        if k & bit:
            value = value + bit - 2 * bit * ((value // bit) % 2)
        bit *= 2
    return value


def low(k):
    return k & -k


def bits_below(limit):
    bit = 1
    while bit < limit:
        yield bit
        bit *= 2


def layer_kernel(n_z, n_y, n_x, cuts, tokens_ref, *refs):
    weights = refs[:9]
    first_gain, conv_taps, conv_gain, second_gain, third_gain = refs[9:14]
    out_ref = refs[14]
    bufs = refs[15:24]
    xgs, hiddens = refs[24:26], refs[26:28]
    (xc, core_out, core_in, side_out, side_in, held, line_out, line_in,
     c_core_out, c_core_in, c_side_out, c_side_in, current, conv_in, acted, stat) = refs[28:44]
    (wz_s, wz_r, wy_s, wy_r, own_s, gz_s, gz_r, gx_s, gx_r, gc_s, gc_r,
     rc_s, rc_r, rx_s, rx_r, rz_s, rz_r, st_s, st_r) = refs[44:]

    n_tp = n_x * CORES
    fs = lax.axis_index("fs")
    tp = lax.axis_index("tp")
    z, y = fs // n_y, fs % n_y
    x, core = tp // CORES, tp % CORES
    length, width = tokens_ref.shape
    features = width * n_tp
    partner = (fs, x * CORES + 1 - core)

    def along(k):
        return (flip(z, k, n_z) * n_y + y, tp)


    barrier = pltpu.get_barrier_semaphore()
    for k in range(1, n_z):
        pl.semaphore_signal(barrier, inc=1, device_id=(flip(z, k, n_z) * n_y + y, tp), device_id_type=MESH)
    for o in range(1, n_y):
        pl.semaphore_signal(barrier, inc=1, device_id=(z * n_y + (y + o) % n_y, tp), device_id_type=MESH)
    for o in range(1, n_tp):
        pl.semaphore_signal(barrier, inc=1, device_id=(fs, (tp + o) % n_tp), device_id_type=MESH)
    pl.semaphore_wait(barrier, n_z - 1 + n_y - 1 + n_tp - 1)

    pending = {}

    def remote(src, dst, s, r, dest):
        return pltpu.make_async_remote_copy(
            src_ref=src, dst_ref=dst, send_sem=s, recv_sem=r, device_id=dest, device_id_type=MESH
        )

    def send(group, src, dst, s, r, dest):
        copy = remote(src, dst, s, r, dest)
        copy.start()
        pending.setdefault(group, []).append(copy)

    def arrive(dst, s, r):
        remote(dst, dst, s, r, (fs, tp)).wait_recv()

    def flush(*groups):
        for group in groups:
            for copy in pending.pop(group, []):
                copy.wait_send()

    def slot(m, block):
        if m in DOWN:
            return bufs[m].at[block]
        rows = bufs[m].shape[0] // (n_z * n_y)
        return bufs[m].at[pl.ds(pl.multiple_of(block * rows, 16), rows)]

    def part_of(m, zz):
        if m in CONV:
            return weights[m]
        place = zz % cuts[m in LAST]
        chunk = hiddens[m in LAST].shape[2]
        if m in DOWN:
            return weights[m].at[pl.ds(pl.multiple_of(place * chunk, 16), chunk)]
        if len(weights[m].shape) == 3:
            return weights[m].at[place]
        return weights[m].at[:, pl.ds(pl.multiple_of(place * chunk, 128), chunk)]

    units = [(m, k, 0) for m in FIRST for k in range(n_z - 1, 0, -1)]
    units += [(m, k, 0) for m in LAST for k in (1, *range(n_z - 1, 1, -1))]
    halved = units[-1][:2]
    units.append((*halved, 1))

    def half(ref, m, k, j):
        if (m, k) != halved:
            return ref
        rows = ref.shape[0] // 2
        return ref.at[pl.ds(j * rows, rows)]

    def z_sems(m, k, j=0):
        i = 9 * (n_z - 1) if j else m * (n_z - 1) + k - 1
        return wz_s.at[i], wz_r.at[i]

    def y_sems(m, k, j, o):
        i = 9 * n_z if j else m * n_z + k
        return wy_s.at[i, o - 1], wy_r.at[i, o - 1]

    def to_y(m, k, src, j=0):
        for o in range(1, n_y):
            dst = half(slot(m, along(k)[0]), m, k, j)
            send("weights", src, dst, *y_sems(m, k, j, o), (z * n_y + (y + o) % n_y, tp))

    def tree_send(group, k, src, dst, s, r):
        for bit in bits_below(low(k) if k else n_z):
            send(group, src, dst, s(k ^ bit), r(k ^ bit), along(bit))

    def weight_own(*matrices):
        for m in matrices:
            own = part_of(m, z)
            to_y(m, 0, own)
            pltpu.make_async_copy(own, slot(m, fs), own_s.at[m]).start()

    def unit_send(m, k, j):
        src = half(part_of(m, flip(z, k, n_z)), m, k, j)
        send("weights", src, half(slot(m, fs), m, k, j), *z_sems(m, k, j), along(k))

    def unit_forward(m, k, j):
        block = half(slot(m, along(k)[0]), m, k, j)
        arrive(block, *z_sems(m, k, j))
        to_y(m, k, block, j)

    def conv_start():
        for m in CONV:
            tree_send("weights", 0, weights[m], slot(m, fs), lambda k: z_sems(m, k)[0], lambda k: z_sems(m, k)[1])
        weight_own(*CONV)

    def conv_block(k):
        for m in CONV:
            block = slot(m, along(k)[0])
            arrive(block, *z_sems(m, k))
            tree_send("weights", k, block, block, lambda i: z_sems(m, i)[0], lambda i: z_sems(m, i)[1])
            to_y(m, k, block)

    def weight_ready(m):
        for k in range(n_z):
            zz = flip(z, k, n_z)
            for o in range(1, n_y):
                block = slot(m, zz * n_y + (y + n_y - o) % n_y)
                for j in range(1 + ((m, k) == halved)):
                    arrive(half(block, m, k, j), *y_sems(m, k, j, o))
        pltpu.make_async_copy(part_of(m, z), slot(m, fs), own_s.at[m]).wait()

    sent, landed = [0], [0]

    def issue(count):
        for unit in units[sent[0] : sent[0] + count]:
            unit_send(*unit)
        sent[0] = min(sent[0] + count, len(units))

    def forward(count):
        for unit in units[landed[0] : landed[0] + count]:
            unit_forward(*unit)
        landed[0] = min(landed[0] + count, len(units))

    def until(*matrices):
        need = 1 + max((n for n, unit in enumerate(units) if unit[0] in matrices), default=-1)
        issue(max(need - sent[0], 0))
        forward(max(need - landed[0], 0))
        for m in matrices:
            weight_ready(m)

    def act(step):
        for fn, *args in step:
            fn(*args)

    def columns(t):
        return pl.ds(pl.multiple_of(t * width, 128), width)

    def spread(group, src, dst, x_s, x_r, c_s, c_r):
        for o in range(1, n_x):
            send(group, src, dst(tp), x_s(o - 1), x_r(o - 1), (fs, (x + o) % n_x * CORES + core))
        send(group, src, dst(tp), c_s(x), c_r(x), partner)

    def pass_on(group, dst, x_s, x_r, c_s, c_r):
        for o in range(1, n_x):
            xx = (x + n_x - o) % n_x
            block = dst(xx * CORES + core)
            arrive(block, x_s(o - 1), x_r(o - 1))
            send(group, block, block, c_s(xx), c_r(xx), partner)

    def collect(dst, x_s, x_r, c_s, c_r):
        for o in range(n_x):
            xx = (x + o) % n_x
            arrive(dst(xx * CORES + 1 - core), c_s(xx), c_r(xx))

    def seq_refs(f, k):
        b = f * n_z + k
        return (
            lambda t: xgs[f].at[k, :, columns(t)],
            lambda i: gx_s.at[b, i], lambda i: gx_r.at[b, i],
            lambda i: gc_s.at[b, i], lambda i: gc_r.at[b, i],
        )

    def line_sems(f, k):
        return gz_s.at[f * (n_z - 1) + k - 1], gz_r.at[f * (n_z - 1) + k - 1]

    def gather_start(f, src):
        group = ("gather", f)
        for bit in bits_below(cuts[f]):
            send(group, src, xgs[f].at[bit, :, columns(tp)], *line_sems(f, bit), along(bit))
        spread(group, src, *seq_refs(f, 0))
        xgs[f][0, :, columns(tp)] = src[...]

    def gather_block(f, k):
        group = ("gather", f)
        block = xgs[f].at[k, :, columns(tp)]
        arrive(block, *line_sems(f, k))
        for bit in bits_below(low(k)):
            send(group, block, xgs[f].at[k ^ bit, :, columns(tp)], *line_sems(f, k ^ bit), along(bit))
        spread(group, block, *seq_refs(f, k))

    def gather_pass(f, k):
        pass_on(("gather", f), *seq_refs(f, k))

    def ffn_hidden(f, k, gate, up):
        rows = xgs[f][k]
        g = jnp.dot(rows, gate[...], preferred_element_type=F32)
        u = jnp.dot(rows, up[...], preferred_element_type=F32)
        hiddens[f][k] = (g * jax.nn.sigmoid(g) * u).astype(BF16)

    def project(source, down, t):
        part = down.shape[2]
        per = width // part
        for q in range(per):
            yield slice(q * part, (q + 1) * part), jnp.dot(source[...], down[t * per + q], preferred_element_type=F32)

    def reduce_give(group, source, down, outgoing, incoming, s, r):
        for o in [*range(1, n_x), 0]:
            xx = (x + o) % n_x
            for cols, value in project(source, down, xx * CORES + 1 - core):
                outgoing(xx)[:, cols] = value.astype(BF16)
            send(group, outgoing(xx), incoming(xx), s(xx), r(xx), partner)

    def reduce_take(group, source, down, incoming, s, r, outgoing, target, xs, xr, keep):
        for o in [*range(1, n_x), 0]:
            xx = (x + o) % n_x
            arrive(incoming(xx), s(xx), r(xx))
            for cols, value in project(source, down, xx * CORES + core):
                total = value + incoming(xx)[:, cols].astype(F32)
                if o:
                    outgoing(o - 1)[:, cols] = total.astype(BF16)
                else:
                    keep[:, cols] = total
            if o:
                send(group, outgoing(o - 1), target(o - 1), xs(o - 1), xr(o - 1), (fs, xx * CORES + core))

    def reduce_sum(target, xs, xr, keep):
        total = keep[...]
        for o in range(1, n_x):
            arrive(target(o - 1), xs(o - 1), xr(o - 1))
            total = total + target(o - 1)[...].astype(F32)
        keep[...] = total

    def reduce_ffn(f, down, plan):
        group = ("reduce", f)

        def give(k):
            reduce_give(
                group, hiddens[f].at[k], down, lambda i: core_out.at[k, i], lambda i: core_in.at[k, i],
                lambda i: rc_s.at[f * n_z + k, i], lambda i: rc_r.at[f * n_z + k, i],
            )

        def take(k):
            reduce_take(
                group, hiddens[f].at[k], down, lambda i: core_in.at[k, i],
                lambda i: rc_s.at[f * n_z + k, i], lambda i: rc_r.at[f * n_z + k, i],
                lambda i: side_out.at[k, i], lambda i: side_in.at[k, i],
                lambda i: rx_s.at[f * n_z + k, i], lambda i: rx_r.at[f * n_z + k, i], held.at[k],
            )

        def line_add(k, i):
            arrive(line_in.at[i], rz_s.at[f * (n_z - 1)], rz_r.at[f * n_z + i])
            held[k] = held[k] + line_in[i].astype(F32)

        def line_copy(k, i, dest):
            return remote(line_out.at[k - 1], line_in.at[i], rz_s.at[f * (n_z - 1) + k - 1], rz_r.at[f * n_z + i], along(dest))

        def line_go(k, i, dest):
            line_out[k - 1] = held[k].astype(BF16)
            line_copy(k, i, dest).start()

        def line_tree(k):
            for bit in bits_below(low(k) if k else cuts[f]):
                line_add(k, (k ^ bit) - 1)
            if k:
                line_go(k, k - 1, low(k))
                pending.setdefault(group, []).append(line_copy(k, k - 1, low(k)))

        def line_inner(k):
            inner = (z + 1) // 2 % 2

            def outer_far():
                line_go(k, 5 - k, 1)

            def inner_near():
                line_add(2, 2)
                line_go(2, 1, 2)

            def inner_far():
                line_add(3, 3)
                line_go(3, 1, 3)

            if k > 1:
                pl.when(inner == 0)(outer_far)
            if k == 2:
                pl.when(inner == 1)(inner_near)
            if k == 1:
                line_go(1, 0, 1)
                pl.when(inner == 1)(inner_far)
            if k == 0:
                line_add(0, 0)
                line_add(0, 1)
            else:
                pending.setdefault(group, []).append(line_copy(k, 0, 1))

        give(cuts[f] - 1)
        for k in range(cuts[f] - 1, -1, -1):
            if k:
                give(k - 1)
            take(k)
        act(plan.get("given", ()))
        for k in range(cuts[f] - 1, -1, -1):
            act(plan.get(k, ()))
            reduce_sum(
                lambda i: side_in.at[k, i], lambda i: rx_s.at[f * n_z + k, i], lambda i: rx_r.at[f * n_z + k, i], held.at[k]
            )
            if cuts[f] == 4:
                line_inner(k)
            else:
                line_tree(k)
        return held[0]

    def stats_start(phase, values):
        sums = jnp.sum(values, axis=-1, keepdims=True)
        squares = jnp.sum(values * values, axis=-1, keepdims=True)
        lane = lax.broadcasted_iota(jnp.int32, (values.shape[0], 128), 1)
        both = jnp.where(lane == 0, sums, jnp.where(lane == 1, squares, 0.0))
        stat[phase, n_tp - 1] = both.T[:8]
        for step in range(1, n_tp):
            i = step - 1
            remote(
                stat.at[phase, n_tp - 1], stat.at[phase, i], st_s.at[phase, i], st_r.at[phase, i],
                (fs, (tp + step) % n_tp),
            ).start()

    def stats_wait(phase, all_width):
        for step in range(1, n_tp):
            i = step - 1
            remote(
                stat.at[phase, n_tp - 1], stat.at[phase, i], st_s.at[phase, i], st_r.at[phase, i], (fs, tp)
            ).wait()
        total = stat[phase, 0]
        for i in range(1, n_tp):
            total = total + stat[phase, i]
        both = jnp.concatenate([total] * 16, axis=0).T
        center = both[:, 0:1] / all_width
        spread_of = both[:, 1:2] / all_width - center * center
        return center, lax.rsqrt(spread_of + EPSILON)

    def row_of(gain):
        return gain[...].astype(F32).reshape(1, gain.shape[0])

    def post_norm(phase, gain):
        stats_start(phase, current[...])
        center, scale = stats_wait(phase, features)
        return ((current[...] - center) * scale * row_of(gain)).astype(BF16)

    gather_start(0, tokens_ref)
    weight_own(*FIRST, *LAST[:2])
    issue(3)
    gather_block(0, 1)
    issue(1)
    gather_block(0, 2)
    issue(2)
    gather_pass(0, 0)
    forward(2)
    gather_block(0, 3)
    issue(3)
    conv_start()
    issue(2)
    gather_pass(0, 1)
    forward(1)
    gather_pass(0, 2)
    forward(1)
    gather_pass(0, 3)
    for k in range(n_z):
        collect(*seq_refs(0, k))
    until(0, 1)
    forward(2)
    for low_k, high_k in ((0, n_z // 2), (n_z // 2, n_z)):
        lax.fori_loop(low_k, high_k, lambda i, c: (ffn_hidden(0, i, bufs[0], bufs[1]), c)[1], 0)
        forward(1 if low_k == 0 else 0)
    until(2)
    current[...] = ALPHA * tokens_ref[...].astype(F32) + 0.5 * reduce_ffn(0, bufs[2], {
        "given": [(conv_block, 1), (conv_block, 2), (issue, 1)],
        2: [(forward, 1)],
        1: [(forward, 1), (weight_own, LAST[2])],
        0: [(issue, 1)],
    })
    issue(1)
    forward(1)
    first = post_norm(0, first_gain)
    out_ref[...] = first

    conv_refs = (
        lambda t: xc.at[:, columns(t)],
        lambda i: gx_s.at[n_z + cuts[1], i], lambda i: gx_r.at[n_z + cuts[1], i],
        lambda i: gc_s.at[n_z + cuts[1], i], lambda i: gc_r.at[n_z + cuts[1], i],
    )
    spread("conv", out_ref, *conv_refs)
    xc[:, columns(tp)] = first
    conv_block(3)
    forward(1)
    issue(2)
    pass_on("conv", *conv_refs)
    until(3, 4)
    collect(*conv_refs)

    channels = acted.shape[1]
    taps = conv_taps.shape[0]
    reach = (taps - 1) // 2
    margin = (conv_in.shape[0] - length) // 2
    rows = xc[...]
    value = jnp.dot(rows, bufs[3][...], preferred_element_type=F32)
    gate = jnp.dot(rows, bufs[4][...], preferred_element_type=F32)
    conv_in[0:margin] = jnp.zeros((margin, channels), F32)
    conv_in[margin + length :] = jnp.zeros((margin, channels), F32)
    conv_in[margin : margin + length] = value * jax.nn.sigmoid(gate)
    rows_each = length // 4
    for top in range(0, length, rows_each):
        for left in range(0, channels, 128):
            cols = slice(left, left + 128)
            total = jnp.zeros((rows_each, 128), F32)
            for tap in range(taps):
                start = margin - reach + top + tap
                total = total + conv_taps[tap : tap + 1, cols].astype(F32) * conv_in[start : start + rows_each, cols]
            current[top : top + rows_each, cols] = total
    stats_start(1, current[:, 0:channels])
    center, scale = stats_wait(1, channels * n_tp)
    normed = (current[:, 0:channels] - center) * scale * row_of(conv_gain)
    acted[...] = (normed * jax.nn.sigmoid(normed)).astype(BF16)
    until(5)
    conv_core = (lambda i: rc_s.at[n_z + cuts[1], i], lambda i: rc_r.at[n_z + cuts[1], i])
    conv_side = (lambda i: rx_s.at[n_z + cuts[1], i], lambda i: rx_r.at[n_z + cuts[1], i])
    reduce_give("conv", acted, bufs[5], lambda i: c_core_out.at[i], lambda i: c_core_in.at[i], *conv_core)
    issue(1)
    reduce_take(
        "conv", acted, bufs[5], lambda i: c_core_in.at[i], *conv_core,
        lambda i: c_side_out.at[i], lambda i: c_side_in.at[i], *conv_side, current,
    )
    forward(1)
    reduce_sum(lambda i: c_side_in.at[i], *conv_side, current)
    current[...] = ALPHA * out_ref[...].astype(F32) + current[...]
    second = post_norm(2, second_gain)
    flush("conv")
    out_ref[...] = second

    gather_start(1, out_ref)
    issue(2)
    forward(2)
    gather_block(1, 1)
    forward(1)
    gather_pass(1, 0)
    until(6, 7)
    collect(*seq_refs(1, 0))
    ffn_hidden(1, 0, bufs[6], bufs[7])
    forward(2)
    for k in range(1, cuts[1]):
        if k > 1:
            gather_block(1, k)
        gather_pass(1, k)
        collect(*seq_refs(1, k))
        ffn_hidden(1, k, bufs[6], bufs[7])
    until(8)
    flush(("reduce", 0))
    current[...] = ALPHA * out_ref[...].astype(F32) + 0.5 * reduce_ffn(1, bufs[8], {})
    normed = post_norm(3, third_gain)
    flush("weights", ("gather", 0), ("gather", 1), ("reduce", 1))
    out_ref[...] = normed


def solution(mesh):
    n_fs, n_tp = mesh.shape["fs"], mesh.shape["tp"]
    n_y = 1 << ((n_fs.bit_length() - 1) // 2)
    n_z, n_x = n_fs // n_y, n_tp // CORES

    def body(
        tokens, first_gate, first_up, first_down, first_gain, glu_value, glu_gate, conv_taps, conv_gain,
        conv_proj, second_gain, last_gate, last_up, last_down, third_gain,
    ):
        tokens = tokens[0]
        length, width = tokens.shape
        features = width * n_tp
        cuts = (n_z, min(n_z, 2))
        chunks = [first_gate.shape[1] // cut for cut in cuts]

        def by_chunk(w, f):
            if chunks[f] % 128 == 0:
                return w
            return jnp.swapaxes(w.reshape(w.shape[0], cuts[f], chunks[f]), 0, 1)

        weights = (
            by_chunk(first_gate, 0), by_chunk(first_up, 0), first_down, glu_value, glu_gate, conv_proj,
            by_chunk(last_gate, 1), by_chunk(last_up, 1), last_down,
        )
        channels = glu_value.shape[1]
        reach = (conv_taps.shape[0] - 1) // 2
        margin = -(-reach // 8) * 8
        part = first_down.shape[1]
        wide = [pltpu.VMEM((features, chunk), BF16) for chunk in chunks]
        down = [pltpu.VMEM((n_fs, chunk, part), BF16) for chunk in chunks]
        glu = pltpu.VMEM((features, channels), BF16)
        proj = pltpu.VMEM((n_fs, channels, part), BF16)
        dma = pltpu.SemaphoreType.DMA
        vmem = pl.BlockSpec(memory_space=pltpu.VMEM)
        others = max(n_x - 1, 1)
        blocks_in_all = n_z + cuts[1] + 1

        def blocks(*lead, kind=BF16):
            return pltpu.VMEM(lead + (length, width), kind)

        def pair(*shape):
            return [dma(shape), dma(shape)]

        result = pl.pallas_call(
            functools.partial(layer_kernel, n_z, n_y, n_x, cuts),
            out_shape=jax.ShapeDtypeStruct((length, width), BF16),
            in_specs=[vmem] + [pl.BlockSpec(memory_space=pl.ANY)] * 9 + [vmem] * 5,
            out_specs=vmem,
            scratch_shapes=[wide[0], wide[0], down[0], glu, glu, proj, wide[1], wide[1], down[1]]
            + [pltpu.VMEM((cut, length, features), BF16) for cut in cuts]
            + [pltpu.VMEM((cut, length, chunk), BF16) for cut, chunk in zip(cuts, chunks)]
            + [
                pltpu.VMEM((length, features), BF16),
                blocks(n_z, n_x),
                blocks(n_z, n_x),
                blocks(n_z, others),
                blocks(n_z, others),
                blocks(n_z, kind=F32),
                blocks(n_z),
                blocks(n_z),
                blocks(n_x),
                blocks(n_x),
                blocks(others),
                blocks(others),
                blocks(kind=F32),
                pltpu.VMEM((length + 2 * margin, channels), F32),
                pltpu.VMEM((length, channels), BF16),
                pltpu.VMEM((4, n_tp, 8, length), F32),
            ]
            + pair(9 * (n_z - 1) + 1)
            + pair(9 * n_z + 1, max(n_y - 1, 1))
            + [dma((9,))]
            + pair(n_z + cuts[1] - 2)
            + pair(blocks_in_all, others)
            + pair(blocks_in_all, n_x)
            + pair(blocks_in_all, n_x)
            + pair(blocks_in_all, others)
            + [dma((n_z + cuts[1] - 2,)), dma((n_z + cuts[1] - 1,))]
            + pair(4, n_tp - 1),
            compiler_params=pltpu.CompilerParams(
                collective_id=0, has_side_effects=True, vmem_limit_bytes=67000000
            ),
        )(
            tokens, *weights, first_gain, conv_taps, conv_gain, second_gain, third_gain
        )
        return result[None]

    weight = P("fs", "tp")
    return jax.shard_map(
        body,
        mesh=mesh,
        in_specs=(
            P("fs", None, "tp"), weight, weight, P("tp", "fs"), P("tp"), weight, weight, P(None, "tp"), P("tp"),
            P("tp", "fs"), P("tp"), weight, weight, P("tp", "fs"), P("tp"),
        ),
        out_specs=P("fs", None, "tp"),
        check_vma=False,
    )
```
